32 devices in a mesh: ep: 16 (over z, y, core), tp: 2 (over x).
Axes of the slice: x: 2, y: 2, z: 4, core: 2. Of those that a mesh axis runs over, the one named last changes fastest.
Arguments:
- tokens: bfloat16 [128, 1024], P('ep'), may hold values from -6 to 6
- ssm_state: float32 [128, 32, 64, 128], P('ep', 'tp'), may hold values from -6 to 6
- conv_x: bfloat16 [128, 3, 2048], P('ep', None, 'tp'), may hold values from -6 to 6
- conv_b: bfloat16 [128, 3, 1024], P('ep', None, 'tp'), may hold values from -6 to 6
- conv_c: bfloat16 [128, 3, 1024], P('ep', None, 'tp'), may hold values from -6 to 6
- w_x: bfloat16 [1024, 2048], P(None, 'tp'), may hold values from -0.1875 to 0.1875
- w_z: bfloat16 [1024, 2048], P(None, 'tp'), may hold values from -0.1875 to 0.1875
- w_b: bfloat16 [1024, 1024], P(None, 'tp'), may hold values from -0.1875 to 0.1875
- w_c: bfloat16 [1024, 1024], P(None, 'tp'), may hold values from -0.1875 to 0.1875
- w_dt: bfloat16 [1024, 32], replicated, may hold values from -0.1875 to 0.1875
- dt_bias: float32 [32], P('tp'), may hold values from -2 to 1
- a_log: float32 [32], P('tp'), may hold values from -3 to 1
- d_skip: float32 [32], P('tp'), may hold values from 0.1 to 1.9
- taps_x: bfloat16 [4, 2048], P(None, 'tp'), may hold values from -3 to 3
- taps_b: bfloat16 [4, 1024], P(None, 'tp'), may hold values from -3 to 3
- taps_c: bfloat16 [4, 1024], P(None, 'tp'), may hold values from -3 to 3
- norm1_gain: float32 [1024], replicated, may hold values from 0.1 to 1.9
- group_gain: float32 [2048], P('tp'), may hold values from 0.1 to 1.9
- w_out: bfloat16 [2048, 1024], P('tp'), may hold values from -0.125 to 0.125
- norm2_gain: float32 [1024], replicated, may hold values from 0.1 to 1.9
- route_ids: int32 [128, 6], P('ep'), may hold values from 0 to 15, all different within a row; in each aligned block of 8 rows (0 to 7, 8 to 15, ...) at most 6 rows name the same one
- route_weights: float32 [128, 6], P('ep'), may hold values from 0.1 to 1
- exp_gate: bfloat16 [16, 1024, 512], P('ep', None, 'tp'), may hold values from -0.1875 to 0.1875
- exp_up: bfloat16 [16, 1024, 512], P('ep', None, 'tp'), may hold values from -0.1875 to 0.1875
- exp_down: bfloat16 [16, 512, 1024], P('ep', 'tp'), may hold values from -0.25 to 0.25
- dense_gate: bfloat16 [1024, 1024], P('ep', 'tp'), may hold values from -0.1875 to 0.1875
- dense_up: bfloat16 [1024, 1024], P('ep', 'tp'), may hold values from -0.1875 to 0.1875
- dense_down: bfloat16 [1024, 1024], P('tp', 'ep'), may hold values from -0.1875 to 0.1875
- branch_gate: bfloat16 [1024], replicated, may hold values from -0.375 to 0.375
Outputs:
- mixed: bfloat16 [128, 1024], P('ep', 'tp')
- state_next: float32 [128, 32, 64, 128], P('ep', 'tp')
- conv_x_next: bfloat16 [128, 3, 2048], P('ep', None, 'tp')
- conv_b_next: bfloat16 [128, 3, 1024], P('ep', None, 'tp')
- conv_c_next: bfloat16 [128, 3, 1024], P('ep', None, 'tp')
The draws below stay inside these ranges and needn't reach their ends.
Inputs may be any that keep to these rules, and one draw needn't show every extreme that they name: `route_ids`: each row names 6 different experts. Among the rows of one device no expert is named by more than 6 rows, a bound that some block reaches.
All inputs are finite; a program needn't handle non-finite values.
Results may differ from the reference program's by a relative error of at most 0.019.
Values may be sent and summed in bfloat16 or wider, within the bound.
A program may use at most 64 MiB of HBM per device.

```python
import math
import jax
import jax.numpy as jnp
import numpy as np
from jax import lax

D = 1024
HEADS = 32
HEAD_DIM = 64
STATE_DIM = 128
CONV_TAPS = 4
EXPERT_FF = 512
DENSE_FF = 1024
TOP_K = 6
SEQ_DEV = 8
INNER = 2048
STATE_COLS = 1024
TOKENS = 128
EXPERTS = 16
CAP = 6
N_EP = 16
N_TP = 2


def steps_of(own_key, dims, pieces, least, top_value):
    level, own = 1.0, jax.random.fold_in(own_key, 6)
    for position, parts in pieces:
        draws = jnp.exp(jax.random.uniform(jax.random.fold_in(own, position), (parts,), jnp.float32, least / len(pieces), top_value / len(pieces)))
        level = level * jnp.repeat(draws, dims[position] // parts).reshape([-1 if axis == position else 1 for axis in range(len(dims))])
    return level


def shared_out(stream_key, own, number, rows, amount, top, most, slope):
    order = jax.random.permutation(stream_key, amount)
    heavy_load, ordinary = shares(amount, rows * top, most, slope, True), shares(amount, rows * top, most, slope, False)
    places = jnp.arange(amount)

    def named(sizes, turn):
        used = int((sizes > 0).sum())
        fixed = max(1, used // 4)
        passed = fixed + (places - fixed + turn * (used - fixed)) % max(1, amount - fixed)
        return jnp.zeros((amount,), jnp.int32).at[order[jnp.where(places < fixed, places, passed)]].set(jnp.asarray(sizes, jnp.int32))

    sizes = jnp.where(number % 4 == 0, named(heavy_load, number // 4), named(ordinary, number - number // 4 - 1))
    mixed = jax.random.permutation(jax.random.fold_in(own, 3), amount)
    source_of, receiver = mixed[0:amount // 2 * 2:2], mixed[1:amount // 2 * 2:2]
    margin = jnp.minimum(sizes[source_of] - 1, most - sizes[receiver]) // 2
    margin = jnp.where((source_of == order[0]) | (receiver == order[0]) | (sizes[receiver] == 0), 0, jnp.maximum(margin, 0))
    passed = jax.random.randint(jax.random.fold_in(own, 4), (amount // 2,), 0, 1 << 20) % (margin + 1)
    sizes = sizes.at[source_of].add(-passed).at[receiver].add(passed)
    items = jnp.searchsorted(jnp.cumsum(sizes), jnp.arange(rows * top), side="right").astype(jnp.int32)
    table = items.reshape(top, rows).T
    table = table[jax.random.permutation(jax.random.fold_in(own, 1), rows)]
    turn = jax.random.randint(jax.random.fold_in(own, 2), (rows, 1), 0, top)
    return jnp.take_along_axis(table, (jnp.arange(top)[None, :] + turn) % top, axis=1)


def shares(count, total, bound, slope, full):
    loads = [(1 << 20) // math.isqrt(standing ** slope) + 1 for standing in range(1, count + 1)]
    largest = bound if full else min(bound, max(-(-total // count), total * loads[0] // sum(loads)))
    least = 1 if total - largest >= count - 1 else 0
    holding, surplus = [largest] + [least] * (count - 1), total - largest - least * (count - 1)
    while surplus > 0:
        candidates = [i for i in range(1, count) if holding[i] < largest] or [i for i in range(1, count) if holding[i] < bound]
        mass, left = sum([loads[i] for i in candidates]), surplus
        for i in candidates:
            extra = min(bound - holding[i], max(1, left * loads[i] // mass), surplus)
            holding[i] = holding[i] + extra
            surplus = surplus - extra
    return np.array(holding)


def scatter_about(own_key, shape, scale, most, pieces=(), kind=jnp.bfloat16):
    drawn = jax.random.normal(own_key, shape, jnp.float32) * scale
    if len(pieces) > 0:
        drawn = steps_of(own_key, shape, pieces, -0.22, 0.18) * drawn
    return jnp.clip(drawn, min=-most, max=most).astype(kind)


def setup_inputs(seed: int = 0) -> dict:
    keys = jax.random.split(jax.random.key(seed), 30)
    tokens = scatter_about(keys[0], (TOKENS, D), 1.0, 6.0, ((0, 16),))
    ssm_state = scatter_about(keys[1], (TOKENS, HEADS, HEAD_DIM, STATE_DIM), 1.0, 6.0, ((0, 16), (1, 2)), jnp.float32)
    conv_x = scatter_about(keys[2], (TOKENS, CONV_TAPS - 1, INNER), 1.0, 6.0, ((0, 16), (2, 2)))
    conv_b = scatter_about(keys[3], (TOKENS, CONV_TAPS - 1, STATE_COLS), 1.0, 6.0, ((0, 16), (2, 2)))
    conv_c = scatter_about(keys[4], (TOKENS, CONV_TAPS - 1, STATE_COLS), 1.0, 6.0, ((0, 16), (2, 2)))
    w_x = scatter_about(keys[5], (D, INNER), D ** -0.5, 0.1875, ((1, 2),))
    w_z = scatter_about(keys[6], (D, INNER), D ** -0.5, 0.1875, ((1, 2),))
    w_b = scatter_about(keys[7], (D, STATE_COLS), D ** -0.5, 0.1875, ((1, 2),))
    w_c = scatter_about(keys[8], (D, STATE_COLS), D ** -0.5, 0.1875, ((1, 2),))
    w_dt = scatter_about(keys[9], (D, HEADS), D ** -0.5, 0.1875)
    dt_bias = jnp.clip(-2.0 + 3.0 * jax.random.uniform(keys[10], (HEADS,), jnp.float32) ** steps_of(keys[10], (HEADS,), ((0, 2),), -0.2, 0.2), -2.0, 1.0)
    a_log = jnp.clip(-3.0 + 4.0 * jax.random.uniform(keys[11], (HEADS,), jnp.float32) ** steps_of(keys[11], (HEADS,), ((0, 2),), -0.2, 0.2), -3.0, 1.0)
    d_skip = jnp.clip(1.0 + 0.18 * jax.random.normal(keys[12], (HEADS,), jnp.float32), 0.1, 1.9)
    taps_x = scatter_about(keys[13], (CONV_TAPS, INNER), CONV_TAPS ** -0.5, 3.0, ((1, 2),))
    taps_b = scatter_about(keys[14], (CONV_TAPS, STATE_COLS), CONV_TAPS ** -0.5, 3.0, ((1, 2),))
    taps_c = scatter_about(keys[15], (CONV_TAPS, STATE_COLS), CONV_TAPS ** -0.5, 3.0, ((1, 2),))
    norm1_gain = jnp.clip(1.0 + 0.18 * jax.random.normal(keys[16], (D,), jnp.float32), 0.1, 1.9)
    group_gain = jnp.clip(1.0 + 0.18 * jax.random.normal(keys[17], (INNER,), jnp.float32), 0.1, 1.9)
    w_out = scatter_about(keys[18], (INNER, D), INNER ** -0.5, 0.125, ((0, 2),))
    norm2_gain = jnp.clip(1.0 + 0.18 * jax.random.normal(keys[19], (D,), jnp.float32), 0.1, 1.9)
    route_ids_keys = jax.random.split(jax.random.fold_in(keys[20], 1), TOKENS // SEQ_DEV)
    route_ids_turns = jax.random.permutation(jax.random.fold_in(keys[20], 3), TOKENS // SEQ_DEV)
    route_ids = jax.vmap(lambda own, number: shared_out(jax.random.fold_in(keys[20], 2), own, number, SEQ_DEV, EXPERTS, TOP_K, CAP, 2))(route_ids_keys, route_ids_turns).reshape((TOKENS, TOP_K))
    route_weights = jnp.clip(0.1 + 0.9 * jax.random.uniform(keys[21], (TOKENS, TOP_K), jnp.float32) ** steps_of(keys[21], (TOKENS, TOP_K), ((0, 16),), -0.2, 0.2), 0.1, 1.0)
    exp_gate = scatter_about(keys[22], (EXPERTS, D, EXPERT_FF), D ** -0.5, 0.1875, ((0, 16), (2, 2)))
    exp_up = scatter_about(keys[23], (EXPERTS, D, EXPERT_FF), D ** -0.5, 0.1875, ((0, 16), (2, 2)))
    exp_down = scatter_about(keys[24], (EXPERTS, EXPERT_FF, D), EXPERT_FF ** -0.5, 0.25, ((0, 16), (1, 2)))
    dense_gate = scatter_about(keys[25], (D, DENSE_FF), D ** -0.5, 0.1875, ((0, 16), (1, 2)))
    dense_up = scatter_about(keys[26], (D, DENSE_FF), D ** -0.5, 0.1875, ((0, 16), (1, 2)))
    dense_down = scatter_about(keys[27], (DENSE_FF, D), DENSE_FF ** -0.5, 0.1875, ((0, 2), (1, 16)))
    branch_gate = scatter_about(keys[28], (D,), (D // 4) ** -0.5, 0.375)
    return dict(tokens=tokens, ssm_state=ssm_state, conv_x=conv_x, conv_b=conv_b, conv_c=conv_c, w_x=w_x, w_z=w_z, w_b=w_b, w_c=w_c, w_dt=w_dt, dt_bias=dt_bias, a_log=a_log, d_skip=d_skip, taps_x=taps_x, taps_b=taps_b, taps_c=taps_c, norm1_gain=norm1_gain, group_gain=group_gain, w_out=w_out, norm2_gain=norm2_gain, route_ids=route_ids, route_weights=route_weights, exp_gate=exp_gate, exp_up=exp_up, exp_down=exp_down, dense_gate=dense_gate, dense_up=dense_up, dense_down=dense_down, branch_gate=branch_gate)


epsilon = 1e-06

def rms_rows(values, gain):
    return values * lax.rsqrt(lax.optimization_barrier(jnp.mean(values * values, axis=-1, keepdims=True)) + epsilon) * gain

def blocked_sum(left, right, blocks):
    width = left.shape[1] // blocks
    total = jnp.zeros((left.shape[0], right.shape[1]), jnp.float32)
    for index in range(blocks):
        partial_term = jnp.dot(left[:, index * width:(index + 1) * width], right[index * width:(index + 1) * width], preferred_element_type=jnp.float32)
        rounded = lax.optimization_barrier(partial_term.astype(jnp.bfloat16))
        total = total + rounded.astype(jnp.float32)
    return total

def short_conv(previous, fresh, taps):
    window = jnp.concatenate((previous, fresh[:, None]), axis=1)
    summed = lax.optimization_barrier(jnp.sum(window.astype(jnp.float32) * taps.astype(jnp.float32)[None], axis=1))
    return (jax.nn.silu(summed), window[:, 1:])

def mixer_core(x_new, z_new, b_new, c_new, dt_raw, ssm_state, conv_x, conv_b, conv_c, dt_bias, a_log, d_skip, taps_x, taps_b, taps_c, group_gain):
    seqs, heads, head_dim, state_dim = ssm_state.shape
    groups = b_new.shape[1] // state_dim
    x_conv, conv_x_next = short_conv(conv_x, x_new, taps_x)
    b_conv, conv_b_next = short_conv(conv_b, b_new, taps_b)
    c_conv, conv_c_next = short_conv(conv_c, c_new, taps_c)
    x_heads = x_conv.reshape(seqs, heads, head_dim)
    b_heads = jnp.repeat(b_conv.reshape(seqs, groups, state_dim), heads // groups, axis=1)
    c_heads = jnp.repeat(c_conv.reshape(seqs, groups, state_dim), heads // groups, axis=1)
    step = jax.nn.softplus(dt_raw + dt_bias)
    decay = jnp.exp(-step * jnp.exp(a_log))
    state_next = decay[:, :, None, None] * ssm_state + (step[:, :, None] * x_heads)[:, :, :, None] * b_heads[:, :, None, :]
    readout = jnp.einsum('shpn,shn->shp', state_next, c_heads, precision=lax.Precision.HIGHEST) + d_skip[None, :, None] * x_heads
    gated = readout.reshape(seqs, heads * head_dim) * jax.nn.silu(z_new.astype(jnp.float32))
    grouped = gated.reshape(seqs, groups, -1)
    grouped = grouped * lax.rsqrt(lax.optimization_barrier(jnp.mean(grouped * grouped, axis=-1, keepdims=True)) + epsilon)
    mixed_heads = (grouped.reshape(seqs, heads * head_dim) * group_gain).astype(jnp.bfloat16)
    return (mixed_heads, state_next, conv_x_next, conv_b_next, conv_c_next)

def reference(tokens, ssm_state, conv_x, conv_b, conv_c, w_x, w_z, w_b, w_c, w_dt, dt_bias, a_log, d_skip, taps_x, taps_b, taps_c, norm1_gain, group_gain, w_out, norm2_gain, route_ids, route_weights, exp_gate, exp_up, exp_down, dense_gate, dense_up, dense_down, branch_gate):
    stream = tokens.astype(jnp.float32)
    normed = rms_rows(stream, norm1_gain).astype(jnp.bfloat16)
    x_new = jnp.dot(normed, w_x, preferred_element_type=jnp.float32).astype(jnp.bfloat16)
    z_new = jnp.dot(normed, w_z, preferred_element_type=jnp.float32).astype(jnp.bfloat16)
    b_new = jnp.dot(normed, w_b, preferred_element_type=jnp.float32).astype(jnp.bfloat16)
    c_new = jnp.dot(normed, w_c, preferred_element_type=jnp.float32).astype(jnp.bfloat16)
    dt_raw = jnp.dot(normed, w_dt, preferred_element_type=jnp.float32)
    mixed_heads, state_next, conv_x_next, conv_b_next, conv_c_next = mixer_core(x_new, z_new, b_new, c_new, dt_raw, ssm_state, conv_x, conv_b, conv_c, dt_bias, a_log, d_skip, taps_x, taps_b, taps_c, group_gain)
    residual = (stream + blocked_sum(mixed_heads, w_out, N_TP)).astype(jnp.bfloat16)
    normed2 = rms_rows(residual.astype(jnp.float32), norm2_gain).astype(jnp.bfloat16)
    expert_iota = jnp.arange(EXPERTS, dtype=jnp.int32)
    matches = route_ids[:, :, None] == expert_iota[None, None, :]
    routed = lax.optimization_barrier(jnp.sum(matches.astype(jnp.int32), axis=1))
    weight_of = lax.optimization_barrier(jnp.sum(jnp.where(matches, route_weights[:, :, None], jnp.float32(0.0)), axis=1))
    blocked = routed.reshape(N_EP, SEQ_DEV, EXPERTS)
    ranked = (jnp.cumsum(blocked, axis=1) - blocked).reshape(TOKENS, EXPERTS)
    token_iota = jnp.arange(TOKENS, dtype=jnp.int32)
    source = token_iota // SEQ_DEV
    total_slots = EXPERTS * N_EP * CAP
    target = expert_iota[None, :] * (N_EP * CAP) + source[:, None] * CAP + ranked
    target = jnp.where(routed > 0, target, total_slots).astype(jnp.int32)
    owners = jnp.broadcast_to(token_iota[:, None], (TOKENS, EXPERTS)).reshape(-1)
    slot_token = jnp.zeros((total_slots,), jnp.int32).at[target.reshape(-1)].set(owners, mode='drop')
    slot_weight = jnp.zeros((total_slots,), jnp.float32).at[target.reshape(-1)].set(weight_of.reshape(-1), mode='drop')

    def run_expert(operands):
        index_rows, gate_weight, up_weight, down_weight = operands
        chosen = normed2[index_rows]
        gate_pre = jnp.dot(chosen, gate_weight, preferred_element_type=jnp.float32)
        up_pre = jnp.dot(chosen, up_weight, preferred_element_type=jnp.float32)
        active = (jax.nn.silu(gate_pre) * up_pre).astype(jnp.bfloat16)
        return blocked_sum(active, down_weight, N_TP).astype(jnp.bfloat16)
    slot_out = lax.map(run_expert, (slot_token.reshape(EXPERTS, N_EP * CAP), exp_gate, exp_up, exp_down))
    expert_sum = jnp.zeros((TOKENS, D), jnp.float32).at[slot_token].add(slot_weight[:, None] * slot_out.reshape(total_slots, D).astype(jnp.float32))
    dense_pre = jnp.dot(normed2, dense_gate, preferred_element_type=jnp.float32)
    dense_lift = jnp.dot(normed2, dense_up, preferred_element_type=jnp.float32)
    dense_active = (jax.nn.silu(dense_pre) * dense_lift).astype(jnp.bfloat16)
    dense_out = blocked_sum(dense_active, dense_down, N_TP)
    branch = jax.nn.sigmoid(jnp.dot(normed2, branch_gate[:, None], preferred_element_type=jnp.float32))
    mixed = (residual.astype(jnp.float32) + expert_sum + branch * dense_out).astype(jnp.bfloat16)
    return (mixed, state_next, conv_x_next, conv_b_next, conv_c_next)
```

```python
import functools

import jax
import jax.numpy as jnp
from jax import lax
from jax.experimental import pallas as pl
from jax.experimental.pallas import tpu as pltpu
from jax.sharding import PartitionSpec as P

epsilon = 1e-06
cores = 2


def rms_rows(values, gain):
    return values * lax.rsqrt(jnp.mean(values * values, axis=-1, keepdims=True) + epsilon) * gain


def partner(index, i, count):
    if count & (count - 1):
        return lax.rem(index + i, count)
    bit = 1
    other = index
    while bit <= i:
        if i & bit:
            other = other + bit * (1 - 2 * lax.rem(lax.div(index, bit), 2))
        bit *= 2
    return other


def source(index, i, count):
    if count & (count - 1):
        return lax.rem(index + count - i, count)
    return partner(index, i, count)


def layer_kernel(
    peers,
    splits,
    share,
    tokens_ref,
    gain1_ref,
    prev_x_ref,
    prev_b_ref,
    prev_c_ref,
    wdt_ref,
    bias_ref,
    a_log_ref,
    skip_ref,
    taps_x_ref,
    taps_b_ref,
    taps_c_ref,
    group_gain_ref,
    gain2_ref,
    ids_ref,
    weights_ref,
    dense_gate_ref,
    dense_up_ref,
    dense_down_ref,
    branch_ref,
    state_hbm,
    wx_hbm,
    wz_hbm,
    wb_hbm,
    wc_hbm,
    w_out_hbm,
    gate_hbm,
    up_hbm,
    down_hbm,
    own_ref,
    returned,
    state,
    next_x_ref,
    next_b_ref,
    next_c_ref,
    wx,
    wz,
    wb,
    wc,
    w_out,
    gate_up,
    down,
    partials,
    features,
    tables,
    stage_ref,
    dense,
    half_out,
    half_in,
    packed,
    load_sem,
    in_sem,
    part_send,
    part_recv,
    feat_send,
    feat_recv,
    pair_send,
    pair_recv,
    half_send,
    half_recv,
    table_send,
    table_recv,
    dense_send,
    dense_recv,
    ret_send,
    ret_recv,
):
    ep = lax.axis_index("ep")
    tp = lax.axis_index("tp")
    everyone = peers * splits
    chips = peers // cores
    me = ep * splits + tp
    chip = ep // cores
    core = lax.rem(ep, cores)
    mate = 1 - core
    seqs, heads, head_dim, state_dim = state.shape
    width = tokens_ref.shape[1]
    groups = wb.shape[1] // state_dim
    per_group = heads // groups
    inner = heads * head_dim
    hidden = down.shape[0]
    part = width // splits

    loads = [
        pltpu.make_async_copy(hbm, vmem, load_sem.at[i])
        for i, (hbm, vmem) in enumerate(
            (
                (wx_hbm, wx),
                (wb_hbm, wb),
                (wc_hbm, wc),
                (wz_hbm, wz),
                (w_out_hbm, w_out),
                (gate_hbm.at[0], gate_up.at[:, pl.ds(0, hidden)]),
                (up_hbm.at[0], gate_up.at[:, pl.ds(hidden, hidden)]),
                (down_hbm.at[0], down),
            )
        )
    ]
    fetch_state = [
        pltpu.make_async_copy(state_hbm.at[s], state.at[s], in_sem.at[s]) for s in range(seqs)
    ]
    for copy in loads[:3] + fetch_state + loads[3:]:
        copy.start()

    barrier = pltpu.get_barrier_semaphore()

    def greet(i, carry):
        other = lax.rem(me + i, everyone)
        pl.semaphore_signal(
            barrier,
            inc=1,
            device_id={"ep": other // splits, "tp": lax.rem(other, splits)},
            device_id_type=pl.DeviceIdType.MESH,
        )
        return carry

    lax.fori_loop(1, everyone, greet, 0)

    def remote(src, dst, send, recv, to_ep, to_tp):
        return pltpu.make_async_remote_copy(
            src_ref=src,
            dst_ref=dst,
            send_sem=send,
            recv_sem=recv,
            device_id={"ep": to_ep, "tp": to_tp},
            device_id_type=pl.DeviceIdType.MESH,
        )

    def part_copy(i, slot):
        return remote(
            partials.at[slot],
            partials.at[slot],
            part_send.at[i],
            part_recv.at[slot],
            ep,
            partner(tp, i, splits),
        )

    def table_copy(i, slot):
        return remote(
            tables.at[lax.rem(slot, cores), slot // cores],
            tables.at[lax.rem(slot, cores), slot // cores],
            table_send.at[i],
            table_recv.at[slot],
            partner(ep, i, peers),
            tp,
        )

    def dense_copy(i, slot):
        other = partner(ep, i, peers)
        return remote(
            stage_ref.at[other], dense.at[slot], dense_send.at[i], dense_recv.at[slot], other, tp
        )

    def feat_copy(i, slot):
        block = features.at[core, slot]
        return remote(
            block,
            block,
            feat_send.at[i],
            feat_recv.at[slot],
            cores * partner(chip, i, chips) + core,
            tp,
        )

    def pair_copy(slot, of):
        block = features.at[of, slot]
        return remote(
            block, block, pair_send.at[slot], pair_recv.at[slot], cores * chip + mate, tp
        )

    half_copy = remote(
        half_out, half_in, half_send.at[0], half_recv.at[0], cores * chip + mate, tp
    )

    def ret_copy(i, j, slot):
        to_chip = partner(chip, i, chips)
        to_tp = partner(tp, j, splits)
        return remote(
            packed.at[to_tp, to_chip],
            returned.at[slot],
            ret_send.at[i * splits + j],
            ret_recv.at[slot],
            cores * to_chip + mate,
            to_tp,
        )

    def project(weights):
        out = jnp.dot(normed, weights, preferred_element_type=jnp.float32)
        return out.astype(jnp.bfloat16).astype(jnp.float32)

    def conv(prev_ref, fresh, taps_ref, next_ref):
        prev = prev_ref[...].astype(jnp.float32)
        taps = taps_ref[...].astype(jnp.float32)
        depth = prev.shape[0]
        summed = prev[0] * taps[0:1]
        for j in range(1, depth):
            summed = summed + prev[j] * taps[j : j + 1]
            next_ref[j - 1] = prev[j].astype(jnp.bfloat16)
        summed = summed + fresh * taps[depth : depth + 1]
        next_ref[depth - 1] = fresh.astype(jnp.bfloat16)
        return jax.nn.silu(summed)

    normed = rms_rows(tokens_ref[...].astype(jnp.float32), gain1_ref[...]).astype(jnp.bfloat16)
    all_dt = lax.dot_general(
        normed, wdt_ref[...], (((1,), (1,)), ((), ())), preferred_element_type=jnp.float32
    )
    dt_raw = all_dt[:, :heads]
    for t in range(1, all_dt.shape[1] // heads):
        dt_raw = jnp.where(tp == t, all_dt[:, t * heads : (t + 1) * heads], dt_raw)
    step = jax.nn.softplus(dt_raw + bias_ref[...])
    decay = jnp.exp(-step * jnp.exp(a_log_ref[...]))
    spread = lax.broadcasted_iota(jnp.int32, (heads, inner), 1) // head_dim
    spread = spread == lax.broadcasted_iota(jnp.int32, (heads, inner), 0)
    per_head = jnp.concatenate((step, jnp.broadcast_to(skip_ref[...], step.shape)), axis=0)
    wide = jnp.dot(
        per_head,
        spread.astype(jnp.float32),
        precision=lax.Precision.HIGHEST,
        preferred_element_type=jnp.float32,
    )

    lanes = lax.broadcasted_iota(jnp.int32, tables.shape[2:], 1)
    table = jnp.zeros(tables.shape[2:], jnp.float32)
    for k in range(ids_ref.shape[1]):
        table = table + jnp.where(lanes == ids_ref[:, k : k + 1], weights_ref[:, k : k + 1], 0.0)
    tables[core, chip] = table
    lane = lax.broadcasted_iota(jnp.int32, stage_ref.shape[1:], 1)
    for owner in range(peers):
        start = owner * share
        base = start // 128 * 128
        block = jnp.zeros(stage_ref.shape[1:], jnp.float32)
        for i, ref in enumerate((dense_gate_ref, dense_up_ref, dense_down_ref)):
            rows = ref[:, base : base + 128].astype(jnp.float32)
            shift = (i * share - (start - base)) % 128
            if shift:
                rows = pltpu.roll(rows, shift, 1)
            block = jnp.where((lane >= i * share) & (lane < (i + 1) * share), rows, block)
        stage_ref[owner] = block.astype(jnp.bfloat16)
    dense[ep] = stage_ref[ep]

    loads[0].wait()
    xs = conv(prev_x_ref, project(wx[...]), taps_x_ref, next_x_ref)
    pl.semaphore_wait(barrier, everyone - 1)
    for i in reversed(range(1, peers)):
        dense_copy(i, ep).start()
    for i in reversed(range(1, peers)):
        table_copy(i, ep).start()

    loads[1].wait()
    bs = conv(prev_b_ref, project(wb[...]), taps_b_ref, next_b_ref)
    loads[2].wait()
    cs = conv(prev_c_ref, project(wc[...]), taps_c_ref, next_c_ref)
    stepped = jnp.transpose(wide[:seqs] * xs)
    cs_high = cs.astype(jnp.bfloat16)
    cs_low = (cs - cs_high.astype(jnp.float32)).astype(jnp.bfloat16)
    cs_pair = jnp.concatenate((cs_high, cs_low), axis=0)

    row = lax.broadcasted_iota(jnp.int32, (seqs, per_group * head_dim), 0)
    read = [jnp.zeros(row.shape, jnp.float32) for _ in range(groups)]
    for s in range(seqs):
        fetch_state[s].wait()
        for g in range(groups):
            span = slice(g * state_dim, (g + 1) * state_dim)
            fresh = []
            for h in range(g * per_group, (g + 1) * per_group):
                new = (
                    decay[s : s + 1, h : h + 1] * state[s, h]
                    + stepped[h * head_dim : (h + 1) * head_dim, s : s + 1] * bs[s : s + 1, span]
                )
                state[s, h] = new
                fresh.append(new.astype(jnp.bfloat16))
            both = lax.dot_general(
                cs_pair[:, span],
                jnp.concatenate(fresh, axis=0),
                (((1,), (1,)), ((), ())),
                preferred_element_type=jnp.float32,
            )
            read[g] = jnp.where(row == s, both[:seqs] + both[seqs:], read[g])
    loads[3].wait()
    gate = jax.nn.silu(project(wz[...]))
    gated = (jnp.concatenate(read, axis=1) + wide[seqs:] * xs) * gate
    block = inner // groups
    mixed_heads = []
    for g in range(groups):
        span = slice(g * block, (g + 1) * block)
        piece = gated[:, span]
        piece = piece * lax.rsqrt(jnp.mean(piece * piece, axis=-1, keepdims=True) + epsilon)
        mixed_heads.append((piece * group_gain_ref[:, span]).astype(jnp.bfloat16))
    loads[4].wait()
    partial_out = jnp.dot(
        jnp.concatenate(mixed_heads, axis=1), w_out[...], preferred_element_type=jnp.float32
    )
    partials[tp] = partial_out.astype(jnp.bfloat16)
    for i in range(1, splits):
        part_copy(i, tp).start()

    for i in range(1, peers):
        table_copy(i, source(ep, i, peers)).wait_recv()
    for i in range(1, peers):
        dense_copy(i, source(ep, i, peers)).wait_recv()
    for load in loads[5:]:
        load.wait()

    for i in range(1, splits):
        part_copy(i, source(tp, i, splits)).wait_recv()
    summed = partials[0].astype(jnp.float32)
    for t in range(1, splits):
        summed = summed + partials[t].astype(jnp.float32)
    residual = (tokens_ref[...].astype(jnp.float32) + summed).astype(jnp.bfloat16)
    residual = residual.astype(jnp.float32)
    features[core, chip] = rms_rows(residual, gain2_ref[...]).astype(jnp.bfloat16)
    for i in reversed(range(1, chips)):
        feat_copy(i, chip).start()
    pair_copy(chip, core).start()

    own_rows = residual[:, :part]
    for t in range(1, splits):
        own_rows = jnp.where(tp == t, residual[:, t * part : (t + 1) * part], own_rows)
    own_ref[...] = own_rows

    for i in range(1, chips):
        slot = source(chip, i, chips)
        feat_copy(i, slot).wait_recv()
        pair_copy(slot, core).start()

    dense_weights = dense[...].reshape(width, dense.shape[2])
    rows_of = chips * seqs

    def feed_forward(of):
        rows16 = features[of].reshape(rows_of, width)
        weights = tables[of].reshape(rows_of, tables.shape[3])
        columns = lax.broadcasted_iota(jnp.int32, weights.shape, 1)
        weight = jnp.sum(jnp.where(columns == ep, weights, 0.0), axis=1, keepdims=True)
        pre = jnp.dot(rows16, gate_up[...], preferred_element_type=jnp.float32)
        active = weight * (jax.nn.silu(pre[:, :hidden]) * pre[:, hidden:])
        dense_pre = jnp.dot(rows16, dense_weights, preferred_element_type=jnp.float32)
        branch = jax.nn.sigmoid(
            jnp.sum(rows16.astype(jnp.float32) * branch_row, axis=1, keepdims=True)
        )
        lane = lax.broadcasted_iota(jnp.int32, dense_pre.shape, 1)
        dense_act = jax.nn.silu(pltpu.roll(dense_pre, 2 * share, 1))
        dense_act = dense_act * pltpu.roll(dense_pre, share, 1)
        dense_act = jnp.where((lane >= 2 * share) & (lane < 3 * share), branch * dense_act, 0.0)
        total = jnp.dot(active.astype(jnp.bfloat16), down[...], preferred_element_type=jnp.float32)
        return total + lax.dot_general(
            dense_act.astype(jnp.bfloat16),
            dense_weights,
            (((1,), (1,)), ((), ())),
            preferred_element_type=jnp.float32,
        )

    branch_row = branch_ref[...].astype(jnp.float32).reshape(1, width)
    half_out[...] = feed_forward(core).astype(jnp.bfloat16)
    half_copy.start()
    for i in range(chips):
        pair_copy(source(chip, i, chips) if i else chip, mate).wait_recv()
    total = feed_forward(mate)
    half_copy.wait_recv()
    total = total + half_in[...].astype(jnp.float32)
    for t in range(splits):
        packed[t] = (
            total[:, t * part : (t + 1) * part].reshape(chips, seqs, part).astype(jnp.bfloat16)
        )
    for i in reversed(range(chips)):
        for j in reversed(range(splits)):
            ret_copy(i, j, chip * splits + tp).start()

    for i in range(1, splits):
        part_copy(i, tp).wait_send()
    for i in range(1, peers):
        table_copy(i, ep).wait_send()
        dense_copy(i, ep).wait_send()
    for i in range(1, chips):
        feat_copy(i, chip).wait_send()
    for i in range(chips):
        pair_copy(source(chip, i, chips) if i else chip, core).wait_send()
    half_copy.wait_send()
    for i in range(chips):
        for j in range(splits):
            slot = (source(chip, i, chips) if i else chip) * splits
            slot = slot + (source(tp, j, splits) if j else tp)
            ret_copy(i, j, slot).wait_recv()
    for i in range(chips):
        for j in range(splits):
            ret_copy(i, j, chip * splits + tp).wait_send()


def finish_kernel(
    own_ref, returned, state, x_ref, b_ref, c_ref, out_ref, state_out, x_out, b_out, c_out, sum_ref, sem
):
    seqs = state.shape[0]
    puts = [pltpu.make_async_copy(state.at[s], state_out.at[s], sem.at[s]) for s in range(seqs)]
    for i, (ref, out) in enumerate(((x_ref, x_out), (b_ref, b_out), (c_ref, c_out))):
        puts.append(pltpu.make_async_copy(ref, out, sem.at[seqs + i]))
    for put in puts:
        put.start()
    mixed = own_ref[...] + jnp.sum(returned[...].astype(jnp.float32), axis=0)
    sum_ref[...] = mixed.astype(jnp.bfloat16)
    last = pltpu.make_async_copy(sum_ref, out_ref, sem.at[seqs + 3])
    last.start()
    for put in puts:
        put.wait()
    last.wait()


def body(
    tokens,
    ssm_state,
    conv_x,
    conv_b,
    conv_c,
    w_x,
    w_z,
    w_b,
    w_c,
    w_dt,
    dt_bias,
    a_log,
    d_skip,
    taps_x,
    taps_b,
    taps_c,
    norm1_gain,
    group_gain,
    w_out,
    norm2_gain,
    route_ids,
    route_weights,
    exp_gate,
    exp_up,
    exp_down,
    dense_gate,
    dense_up,
    dense_down,
    branch_gate,
):
    peers = lax.axis_size("ep")
    splits = lax.axis_size("tp")
    chips = peers // cores
    seqs, width = tokens.shape
    depth, local_hidden = dense_gate.shape
    share = local_hidden // peers
    hidden = exp_gate.shape[2]
    part = width // splits
    lanes = -(-3 * share // 128) * 128
    vmem = pl.BlockSpec(memory_space=pltpu.VMEM)
    hbm = pl.BlockSpec(memory_space=pltpu.HBM)
    dma = lambda count: pltpu.SemaphoreType.DMA((count,))
    taps_first = lambda a: a.transpose(1, 0, 2)
    conv_x, conv_b, conv_c = taps_first(conv_x), taps_first(conv_b), taps_first(conv_c)
    bf16, f32 = jnp.bfloat16, jnp.float32
    in_hbm = lambda a: pltpu.with_memory_space_constraint(a, pltpu.HBM)
    held = pl.pallas_call(
        functools.partial(layer_kernel, peers, splits, share),
        out_shape=(
            pltpu.VMEM((seqs, part), f32),
            pltpu.VMEM((chips * splits, seqs, part), bf16),
            pltpu.VMEM(ssm_state.shape, f32),
            pltpu.VMEM(conv_x.shape, bf16),
            pltpu.VMEM(conv_b.shape, bf16),
            pltpu.VMEM(conv_c.shape, bf16),
        ),
        in_specs=[vmem] * 20 + [hbm] * 9,
        out_specs=(vmem,) * 6,
        scratch_shapes=[
            pltpu.VMEM(w_x.shape, bf16),
            pltpu.VMEM(w_z.shape, bf16),
            pltpu.VMEM(w_b.shape, bf16),
            pltpu.VMEM(w_c.shape, bf16),
            pltpu.VMEM(w_out.shape, bf16),
            pltpu.VMEM((width, 2 * hidden), bf16),
            pltpu.VMEM((hidden, width), bf16),
            pltpu.VMEM((splits, seqs, width), bf16),
            pltpu.VMEM((cores, chips, seqs, width), bf16),
            pltpu.VMEM((cores, chips, seqs, 128), f32),
            pltpu.VMEM((peers, depth, lanes), bf16),
            pltpu.VMEM((peers, depth, lanes), bf16),
            pltpu.VMEM((chips * seqs, width), bf16),
            pltpu.VMEM((chips * seqs, width), bf16),
            pltpu.VMEM((splits, chips, seqs, part), bf16),
            dma(8),
            dma(seqs),
            dma(splits),
            dma(splits),
            dma(chips),
            dma(chips),
            dma(chips),
            dma(chips),
            dma(1),
            dma(1),
            dma(peers),
            dma(peers),
            dma(peers),
            dma(peers),
            dma(chips * splits),
            dma(chips * splits),
        ],
        compiler_params=pltpu.CompilerParams(
            collective_id=0, has_side_effects=True, vmem_limit_bytes=40 * 2**20
        ),
        cost_estimate=pl.CostEstimate(flops=10**9, bytes_accessed=2 * 10**7, transcendentals=0),
    )(*map(in_hbm, (
        tokens,
        norm1_gain[None],
        conv_x,
        conv_b,
        conv_c,
        w_dt.T,
        dt_bias[None],
        a_log[None],
        d_skip[None],
        taps_x,
        taps_b,
        taps_c,
        group_gain[None],
        norm2_gain[None],
        route_ids,
        route_weights,
        dense_gate,
        dense_up,
        dense_down.T,
        branch_gate,
        ssm_state,
        w_x,
        w_z,
        w_b,
        w_c,
        w_out,
        exp_gate,
        exp_up,
        exp_down,
    )))
    held = [pltpu.with_memory_space_constraint(a, pltpu.VMEM) for a in held]
    shape = jax.ShapeDtypeStruct
    mixed, state, next_x, next_b, next_c = pl.pallas_call(
        finish_kernel,
        out_shape=(
            shape((seqs, part), bf16),
            shape(ssm_state.shape, f32),
            shape(conv_x.shape, bf16),
            shape(conv_b.shape, bf16),
            shape(conv_c.shape, bf16),
        ),
        in_specs=[vmem] * 6,
        out_specs=(hbm,) * 5,
        scratch_shapes=[pltpu.VMEM((seqs, part), bf16), dma(seqs + 4)],
        compiler_params=pltpu.CompilerParams(vmem_limit_bytes=8 * 2**20),
        cost_estimate=pl.CostEstimate(flops=10**5, bytes_accessed=5 * 10**6, transcendentals=0),
    )(*held)
    return mixed, state, taps_first(next_x), taps_first(next_b), taps_first(next_c)


def solution(mesh):
    return jax.shard_map(
        body,
        mesh=mesh,
        in_specs=(
            P("ep", None),
            P("ep", "tp", None, None),
            P("ep", None, "tp"),
            P("ep", None, "tp"),
            P("ep", None, "tp"),
            P(None, "tp"),
            P(None, "tp"),
            P(None, "tp"),
            P(None, "tp"),
            P(),
            P("tp"),
            P("tp"),
            P("tp"),
            P(None, "tp"),
            P(None, "tp"),
            P(None, "tp"),
            P(),
            P("tp"),
            P("tp", None),
            P(),
            P("ep", None),
            P("ep", None),
            P("ep", None, "tp"),
            P("ep", None, "tp"),
            P("ep", "tp", None),
            P("ep", "tp"),
            P("ep", "tp"),
            P("tp", "ep"),
            P(),
        ),
        out_specs=(
            P("ep", "tp"),
            P("ep", "tp", None, None),
            P("ep", None, "tp"),
            P("ep", None, "tp"),
            P("ep", None, "tp"),
        ),
        check_vma=False,
    )
```

```python
import functools

import jax
import jax.numpy as jnp
from jax import lax
from jax.experimental import pallas as pl
from jax.experimental.pallas import tpu as pltpu
from jax.sharding import PartitionSpec as P

epsilon = 1e-06
cores = 2


def rms_rows(values, gain):
    return values * lax.rsqrt(jnp.mean(values * values, axis=-1, keepdims=True) + epsilon) * gain


def partner(index, i, count):
    if count & (count - 1):
        return lax.rem(index + i, count)
    bit = 1
    other = index
    while bit <= i:
        if i & bit:
            other = other + bit * (1 - 2 * lax.rem(lax.div(index, bit), 2))
        bit *= 2
    return other


def source(index, i, count):
    if count & (count - 1):
        return lax.rem(index + count - i, count)
    return partner(index, i, count)


def layer_kernel(
    peers,
    splits,
    share,
    fold,
    tokens_hbm,
    gain1_hbm,
    prev_x_hbm,
    prev_b_hbm,
    prev_c_hbm,
    wdt_hbm,
    bias_hbm,
    a_log_hbm,
    skip_hbm,
    taps_x_hbm,
    taps_b_hbm,
    taps_c_hbm,
    group_gain_hbm,
    gain2_hbm,
    ids_hbm,
    weights_hbm,
    dense_gate_hbm,
    dense_up_hbm,
    dense_down_hbm,
    branch_hbm,
    state_hbm,
    wx_hbm,
    wz_hbm,
    wb_hbm,
    wc_hbm,
    w_out_hbm,
    gate_hbm,
    up_hbm,
    down_hbm,
    own_ref,
    returned,
    state,
    next_x_ref,
    next_b_ref,
    next_c_ref,
    tokens_ref,
    gain1_ref,
    wdt_ref,
    bias_ref,
    a_log_ref,
    skip_ref,
    prev_x_ref,
    prev_b_ref,
    prev_c_ref,
    taps_x_ref,
    taps_b_ref,
    taps_c_ref,
    group_gain_ref,
    gain2_ref,
    ids_ref,
    weights_ref,
    branch_ref,
    slabs,
    wx,
    wz,
    wb,
    wc,
    w_out,
    gate_up,
    down,
    decays,
    partials,
    features,
    stage_ref,
    arrived,
    dense,
    half_out,
    half_in,
    packed,
    small_sem,
    load_sem,
    in_sem,
    send_sem,
    part_recv,
    feat_recv,
    batch_recv,
):
    ep = lax.axis_index("ep")
    tp = lax.axis_index("tp")
    everyone = peers * splits
    chips = peers // cores
    me = ep * splits + tp
    chip = ep // cores
    core = lax.rem(ep, cores)
    mate = 1 - core
    seqs, heads, head_dim, state_dim = state.shape
    width = tokens_ref.shape[1]
    groups = wb.shape[1] // state_dim
    per_group = heads // groups
    inner = heads * head_dim
    hidden = down.shape[0]
    part = width // splits
    depth = slabs.shape[1]

    small = {
        name: pltpu.make_async_copy(hbm, vmem, small_sem.at[i])
        for i, (name, hbm, vmem) in enumerate(
            (
                ("tokens", tokens_hbm, tokens_ref),
                ("gain1", gain1_hbm, gain1_ref),
                ("wdt", wdt_hbm, wdt_ref),
                ("bias", bias_hbm, bias_ref),
                ("a_log", a_log_hbm, a_log_ref),
                ("skip", skip_hbm, skip_ref),
                ("prev_x", prev_x_hbm, prev_x_ref),
                ("taps_x", taps_x_hbm, taps_x_ref),
                ("prev_b", prev_b_hbm, prev_b_ref),
                ("taps_b", taps_b_hbm, taps_b_ref),
                ("prev_c", prev_c_hbm, prev_c_ref),
                ("taps_c", taps_c_hbm, taps_c_ref),
                ("group_gain", group_gain_hbm, group_gain_ref),
                ("gain2", gain2_hbm, gain2_ref),
                ("ids", ids_hbm, ids_ref),
                ("weights", weights_hbm, weights_ref),
                ("branch", branch_hbm, branch_ref),
            )
        )
    }

    def ready(*names):
        for name in names:
            small[name].wait()

    loads = [
        pltpu.make_async_copy(hbm, vmem, load_sem.at[i])
        for i, hbm, vmem in (
            (0, wx_hbm, wx),
            (1, wb_hbm, wb),
            (2, wc_hbm, wc),
            (3, wz_hbm, wz),
            (4, w_out_hbm, w_out),
            (5, gate_hbm.at[0], gate_up.at[:, pl.ds(0, hidden)]),
            (5, up_hbm.at[0], gate_up.at[:, pl.ds(hidden, hidden)]),
            (6, down_hbm.at[0], down),
            (7, dense_gate_hbm, slabs.at[0]),
            (7, dense_up_hbm, slabs.at[1]),
            (7, dense_down_hbm, slabs.at[2]),
        )
    ]
    fetch_state = [
        pltpu.make_async_copy(
            state_hbm.at[pl.ds(s, 2)], state.at[pl.ds(s, 2)], in_sem.at[s // 2]
        )
        for s in range(0, seqs, 2)
    ]
    for name in ("tokens", "gain1", "wdt", "bias", "a_log", "skip"):
        small[name].start()
    for copy in loads[8:] + loads[:1]:
        copy.start()
    for name in ("prev_x", "taps_x", "prev_b", "taps_b", "prev_c", "taps_c"):
        small[name].start()
    for copy in loads[1:3]:
        copy.start()
    for name in ("group_gain", "gain2", "ids", "weights", "branch"):
        small[name].start()

    barrier = pltpu.get_barrier_semaphore()

    def greet(to_ep, to_tp):
        pl.semaphore_signal(
            barrier,
            inc=1,
            device_id={"ep": to_ep, "tp": to_tp},
            device_id_type=pl.DeviceIdType.MESH,
        )

    for i in reversed(range(peers)):
        for j in range(splits):
            if i or j:
                greet(partner(ep, i, peers) if i else ep, partner(tp, j, splits) if j else tp)

    def remote(src, dst, send, recv, to_ep, to_tp):
        return pltpu.make_async_remote_copy(
            src_ref=src,
            dst_ref=dst,
            send_sem=send,
            recv_sem=recv,
            device_id={"ep": to_ep, "tp": to_tp},
            device_id_type=pl.DeviceIdType.MESH,
        )

    mate_ep = cores * chip + mate

    def part_copy(i, slot):
        return remote(
            partials.at[slot],
            partials.at[slot],
            send_sem.at[0],
            part_recv.at[slot],
            ep,
            partner(tp, i, splits),
        )

    def dense_copy(i):
        other = partner(ep, i, peers)
        return remote(
            stage_ref.at[other], arrived.at[ep], send_sem.at[1], batch_recv.at[0], other, tp
        )

    def feat_copy(i, slot):
        block = features.at[core, slot]
        return remote(
            block,
            block,
            send_sem.at[2],
            feat_recv.at[slot],
            cores * partner(chip, i, chips) + core,
            tp,
        )

    def pair_copy(slot):
        block = features.at[core, slot]
        return remote(block, block, send_sem.at[3], batch_recv.at[1], mate_ep, tp)

    half_copy = remote(half_out, half_in, send_sem.at[4], batch_recv.at[2], mate_ep, tp)

    def ret_copy(i, j):
        to_chip = partner(chip, i, chips) if i else chip
        to_tp = partner(tp, j, splits) if j else tp
        return remote(
            packed.at[to_tp, to_chip],
            returned.at[chip * splits + tp],
            send_sem.at[5],
            batch_recv.at[3],
            cores * to_chip + mate,
            to_tp,
        )

    def batch(ref, send, recv):
        return remote(ref, ref, send_sem.at[send], batch_recv.at[recv], mate_ep, tp)

    parts_out = remote(
        partials.at[pl.ds(0, splits - 1)],
        partials.at[pl.ds(0, splits - 1)],
        send_sem.at[0],
        part_recv.at[0],
        mate_ep,
        tp,
    )
    dense_all = batch(arrived.at[pl.ds(0, peers - 1)], 1, 0)
    feats_out = batch(features.at[0, pl.ds(0, chips - 1)], 2, 1)
    pairs_all = batch(features.at[mate], 3, 1)
    rets_all = batch(returned, 5, 3)

    def project(weights):
        out = jnp.dot(normed, weights, preferred_element_type=jnp.float32)
        return out.astype(jnp.bfloat16).astype(jnp.float32)

    def conv(prev_ref, fresh, taps_ref, next_ref):
        prev = prev_ref[...].astype(jnp.float32)
        taps = taps_ref[...].astype(jnp.float32)
        count = prev.shape[0]
        summed = prev[0] * taps[0:1]
        for j in range(1, count):
            summed = summed + prev[j] * taps[j : j + 1]
            next_ref[j - 1] = prev[j].astype(jnp.bfloat16)
        summed = summed + fresh * taps[count : count + 1]
        next_ref[count - 1] = fresh.astype(jnp.bfloat16)
        return jax.nn.silu(summed)

    high = lambda a: a.astype(jnp.bfloat16).astype(jnp.float32)
    late = 2 * ep >= peers

    def spread_dense():
        pl.semaphore_wait(barrier, everyone - 1)
        for i in reversed(range(1, peers)):
            dense_copy(i).start()

    ready("tokens", "gain1", "wdt", "bias", "a_log", "skip")
    for copy in fetch_state[: seqs // 4]:
        copy.start()
    normed = rms_rows(tokens_ref[...].astype(jnp.float32), gain1_ref[...]).astype(jnp.bfloat16)
    all_dt = lax.dot_general(
        normed, wdt_ref[...], (((1,), (1,)), ((), ())), preferred_element_type=jnp.float32
    )
    dt_raw = all_dt[:, :heads]
    for t in range(1, all_dt.shape[1] // heads):
        dt_raw = jnp.where(tp == t, all_dt[:, t * heads : (t + 1) * heads], dt_raw)
    step = jax.nn.softplus(dt_raw + bias_ref[...])
    decay = jnp.exp(-step * jnp.exp(a_log_ref[...]))
    for h in range(heads):
        decays[h] = jnp.broadcast_to(decay[:, h : h + 1], (seqs, state_dim))
    spread = lax.broadcasted_iota(jnp.int32, (heads, inner), 1) // head_dim
    spread = spread == lax.broadcasted_iota(jnp.int32, (heads, inner), 0)
    per_head = jnp.concatenate(
        (step, jnp.broadcast_to(skip_ref[...], step.shape), decay), axis=0
    )
    top = high(per_head)
    middle = high(per_head - top)
    pieces = jnp.concatenate((top, middle, per_head - top - middle), axis=0).astype(jnp.bfloat16)
    wide = jnp.dot(pieces, spread.astype(jnp.bfloat16), preferred_element_type=jnp.float32)
    wide = wide[: 3 * seqs] + wide[3 * seqs : 6 * seqs] + wide[6 * seqs :]

    for copy in fetch_state[seqs // 4 :]:
        copy.start()
    pltpu.make_async_copy(slabs, slabs, load_sem.at[7]).wait()
    rows = depth // fold
    lane = lax.broadcasted_iota(jnp.int32, (rows, stage_ref.shape[2]), 1)
    for owner in range(peers):
        start = owner * share
        base = start // 128 * 128
        block = []
        for a in range(3):
            found = jnp.zeros(lane.shape, jnp.float32)
            for q in range(fold):
                at = (q if fold > 1 else a) * share
                piece = slabs[a, q * rows : (q + 1) * rows, base : base + 128].astype(jnp.float32)
                shift = (at - (start - base)) % 128
                if shift:
                    piece = pltpu.roll(piece, shift, 1)
                found = jnp.where((lane >= at) & (lane < at + share), piece, found)
            block.append(found)
        if fold > 1:
            for a in range(3):
                stage_ref[owner, a * rows : (a + 1) * rows] = block[a].astype(jnp.bfloat16)
        else:
            stage_ref[owner] = (block[0] + block[1] + block[2]).astype(jnp.bfloat16)
    arrived[ep] = stage_ref[ep]

    loads[0].wait()
    ready("prev_x", "taps_x")
    xs = conv(prev_x_ref, project(wx[...]), taps_x_ref, next_x_ref)
    loads[3].start()
    pl.when(late)(spread_dense)
    loads[1].wait()
    ready("prev_b", "taps_b")
    bs = conv(prev_b_ref, project(wb[...]), taps_b_ref, next_b_ref)
    loads[2].wait()
    ready("prev_c", "taps_c")
    cs = conv(prev_c_ref, project(wc[...]), taps_c_ref, next_c_ref)
    stepped = wide[:seqs] * xs
    stepped_high = high(stepped)
    left = jnp.transpose(
        jnp.concatenate((stepped_high, stepped - stepped_high, stepped_high), axis=0)
    ).astype(jnp.bfloat16)
    bs_high = high(bs)
    right = jnp.concatenate((bs_high, bs_high, bs - bs_high), axis=0)
    cs_high = high(cs)
    turned = jnp.transpose(jnp.concatenate((cs_high, cs - cs_high), axis=0))
    turned_column = lax.rem(lax.broadcasted_iota(jnp.int32, (state_dim, 2 * seqs), 1), seqs)
    right_row = lax.rem(lax.broadcasted_iota(jnp.int32, (3 * seqs, state_dim), 0), seqs)
    block = per_group * head_dim
    read = [jnp.zeros((block, 2 * seqs), jnp.float32) for _ in range(groups)]
    for s0 in range(0, seqs, 2):
        pair = (s0, s0 + 1)
        if s0 == 2:
            loads[4].start()
        if s0 == seqs // 2:
            for copy in loads[5:8]:
                copy.start()
        fetch_state[s0 // 2].wait()
        for g in range(groups):
            span = slice(g * state_dim, (g + 1) * state_dim)
            old = [state[s, g * per_group : (g + 1) * per_group] for s in pair]
            readers = [jnp.where(turned_column == s, turned[span], 0.0) for s in pair]
            read[g] = read[g] + jnp.dot(
                jnp.concatenate(
                    [a.reshape(block, state_dim).astype(jnp.bfloat16) for a in old], axis=1
                ),
                jnp.concatenate(readers, axis=0).astype(jnp.bfloat16),
                preferred_element_type=jnp.float32,
            )
            adders = [jnp.where(right_row == s, right[:, span], 0.0) for s in pair]
            added = jnp.dot(
                left[g * block : (g + 1) * block],
                jnp.concatenate(adders, axis=1).astype(jnp.bfloat16),
                preferred_element_type=jnp.float32,
            )
            for k, s in enumerate(pair):
                for j in range(per_group):
                    h = g * per_group + j
                    state[s, h] = (
                        decays[h, s : s + 1] * old[k][j]
                        + added[
                            j * head_dim : (j + 1) * head_dim, k * state_dim : (k + 1) * state_dim
                        ]
                    )
    pl.when(jnp.logical_not(late))(spread_dense)
    turned = jnp.transpose(jnp.concatenate(read, axis=0))
    met = []
    for g in range(groups):
        span = slice(g * state_dim, (g + 1) * state_dim)
        dots = jnp.sum(bs[:, span] * cs[:, span], axis=1, keepdims=True)
        met.append(jnp.broadcast_to(dots, (seqs, block)))
    readout = wide[2 * seqs :] * (turned[:seqs] + turned[seqs:])
    readout = readout + stepped * jnp.concatenate(met, axis=1)
    loads[3].wait()
    gate = jax.nn.silu(project(wz[...]))
    gated = (readout + wide[seqs : 2 * seqs] * xs) * gate
    ready("group_gain", "gain2", "ids", "weights", "branch")
    block = inner // groups
    mixed_heads = []
    for g in range(groups):
        span = slice(g * block, (g + 1) * block)
        piece = gated[:, span]
        piece = piece * lax.rsqrt(jnp.mean(piece * piece, axis=-1, keepdims=True) + epsilon)
        mixed_heads.append((piece * group_gain_ref[:, span]).astype(jnp.bfloat16))
    loads[4].wait()
    partial_out = jnp.dot(
        jnp.concatenate(mixed_heads, axis=1), w_out[...], preferred_element_type=jnp.float32
    )
    partials[tp] = partial_out.astype(jnp.bfloat16)
    for i in range(1, splits):
        part_copy(i, tp).start()

    tail = features.shape[3] - width
    lanes = lax.broadcasted_iota(jnp.int32, (seqs, tail), 1)
    table = jnp.zeros((seqs, tail), jnp.float32)
    for k in range(ids_ref.shape[1]):
        table = table + jnp.where(
            lax.rem(lanes, peers) == ids_ref[:, k : k + 1], weights_ref[:, k : k + 1], 0.0
        )
    table = jnp.where(lanes < peers, high(table), table - high(table))
    features[core, chip, :, width:] = table.astype(jnp.bfloat16)

    for i in range(1, splits):
        part_copy(i, source(tp, i, splits)).wait_recv()
    summed = partials[0].astype(jnp.float32)
    for t in range(1, splits):
        summed = summed + partials[t].astype(jnp.float32)
    residual = (tokens_ref[...].astype(jnp.float32) + summed).astype(jnp.bfloat16)
    residual = residual.astype(jnp.float32)
    features[core, chip, :, :width] = rms_rows(residual, gain2_ref[...]).astype(jnp.bfloat16)
    for i in reversed(range(1, chips)):
        feat_copy(i, chip).start()
    pair_copy(chip).start()

    own_rows = residual[:, :part]
    for t in range(1, splits):
        own_rows = jnp.where(tp == t, residual[:, t * part : (t + 1) * part], own_rows)
    own_ref[...] = own_rows

    def collect(first, last):
        for i in range(first, last):
            slot = source(chip, i, chips)
            feat_copy(i, slot).wait_recv()
            pair_copy(slot).start()

    collect(1, chips // 2)
    dense_all.wait_recv()
    if fold > 1:
        for s in range(peers):
            for q in range(fold):
                found = jnp.zeros(lane.shape, jnp.float32)
                for a in range(3):
                    piece = arrived[s, a * rows : (a + 1) * rows].astype(jnp.float32)
                    shift = (a - q) * share % 128
                    if shift:
                        piece = pltpu.roll(piece, shift, 1)
                    found = jnp.where(
                        (lane >= a * share) & (lane < (a + 1) * share), piece, found
                    )
                at = s * depth + q * rows
                dense[at : at + rows] = found.astype(jnp.bfloat16)
        dense_weights = dense[...]
    else:
        dense_weights = arrived[...].reshape(width, arrived.shape[2])
    collect(chips // 2, chips)
    pltpu.make_async_copy(gate_up, gate_up, load_sem.at[5]).wait()
    loads[7].wait()
    rows_of = chips * seqs
    branch_row = branch_ref[...].astype(jnp.float32).reshape(1, width)

    def feed_forward(of):
        rows16 = features[of, :, :, :width].reshape(rows_of, width)
        weights = features[of, :, :, width:].reshape(rows_of, tail).astype(jnp.float32)
        columns = lax.broadcasted_iota(jnp.int32, weights.shape, 1)
        columns = (columns == ep) | (columns == ep + peers)
        weight = jnp.sum(jnp.where(columns, weights, 0.0), axis=1, keepdims=True)
        pre = jnp.dot(rows16, gate_up[...], preferred_element_type=jnp.float32)
        active = weight * (jax.nn.silu(pre[:, :hidden]) * pre[:, hidden:])
        dense_pre = jnp.dot(rows16, dense_weights, preferred_element_type=jnp.float32)
        branch = jax.nn.sigmoid(
            jnp.sum(rows16.astype(jnp.float32) * branch_row, axis=1, keepdims=True)
        )
        lane = lax.broadcasted_iota(jnp.int32, dense_pre.shape, 1)
        dense_act = jax.nn.silu(pltpu.roll(dense_pre, 2 * share, 1))
        dense_act = dense_act * pltpu.roll(dense_pre, share, 1)
        dense_act = jnp.where((lane >= 2 * share) & (lane < 3 * share), branch * dense_act, 0.0)
        total = jnp.dot(active.astype(jnp.bfloat16), down[...], preferred_element_type=jnp.float32)
        return total + lax.dot_general(
            dense_act.astype(jnp.bfloat16),
            dense_weights,
            (((1,), (1,)), ((), ())),
            preferred_element_type=jnp.float32,
        )

    half_out[...] = feed_forward(core).astype(jnp.bfloat16)
    half_copy.start()
    pairs_all.wait_recv()
    total = feed_forward(mate)
    half_copy.wait_recv()
    total = total + half_in[...].astype(jnp.float32)
    for t in range(splits):
        packed[t] = (
            total[:, t * part : (t + 1) * part].reshape(chips, seqs, part).astype(jnp.bfloat16)
        )
    for i in reversed(range(chips)):
        for j in reversed(range(splits)):
            ret_copy(i, j).start()

    parts_out.wait_send()
    dense_all.wait_send()
    feats_out.wait_send()
    pairs_all.wait_send()
    half_copy.wait_send()
    rets_all.wait_recv()
    rets_all.wait_send()


def finish_kernel(
    own_ref, returned, state, x_ref, b_ref, c_ref, out_ref, state_out, x_out, b_out, c_out, sum_ref, sem
):
    seqs = state.shape[0]
    for s in range(seqs):
        pltpu.make_async_copy(state.at[s], state_out.at[s], sem.at[0]).start()
    puts = [pltpu.make_async_copy(state, state_out, sem.at[0])]
    for i, (ref, out) in enumerate(((x_ref, x_out), (b_ref, b_out), (c_ref, c_out))):
        puts.append(pltpu.make_async_copy(ref, out, sem.at[1 + i]))
        puts[-1].start()
    mixed = own_ref[...] + jnp.sum(returned[...].astype(jnp.float32), axis=0)
    sum_ref[...] = mixed.astype(jnp.bfloat16)
    puts.append(pltpu.make_async_copy(sum_ref, out_ref, sem.at[4]))
    puts[-1].start()
    for put in puts:
        put.wait()


def body(
    tokens,
    ssm_state,
    conv_x,
    conv_b,
    conv_c,
    w_x,
    w_z,
    w_b,
    w_c,
    w_dt,
    dt_bias,
    a_log,
    d_skip,
    taps_x,
    taps_b,
    taps_c,
    norm1_gain,
    group_gain,
    w_out,
    norm2_gain,
    route_ids,
    route_weights,
    exp_gate,
    exp_up,
    exp_down,
    dense_gate,
    dense_up,
    dense_down,
    branch_gate,
):
    peers = lax.axis_size("ep")
    splits = lax.axis_size("tp")
    chips = peers // cores
    seqs, width = tokens.shape
    depth, local_hidden = dense_gate.shape
    share = local_hidden // peers
    hidden = exp_gate.shape[2]
    part = width // splits
    heads, state_dim = ssm_state.shape[1], ssm_state.shape[3]
    fold = 128 // share
    if share * fold != 128 or depth % (16 * fold):
        fold = 1
    slab = (peers, 3 * depth // fold if fold > 1 else depth, 128)
    tail = -(-2 * peers // 128) * 128
    vmem = pl.BlockSpec(memory_space=pltpu.VMEM)
    hbm = pl.BlockSpec(memory_space=pltpu.HBM)
    dma = lambda count: pltpu.SemaphoreType.DMA((count,))
    taps_first = lambda a: a.transpose(1, 0, 2)
    conv_x, conv_b, conv_c = taps_first(conv_x), taps_first(conv_b), taps_first(conv_c)
    bf16, f32 = jnp.bfloat16, jnp.float32
    in_hbm = lambda a: pltpu.with_memory_space_constraint(a, pltpu.HBM)
    held = pl.pallas_call(
        functools.partial(layer_kernel, peers, splits, share, fold),
        out_shape=(
            pltpu.VMEM((seqs, part), f32),
            pltpu.VMEM((chips * splits, seqs, part), bf16),
            pltpu.VMEM(ssm_state.shape, f32),
            pltpu.VMEM(conv_x.shape, bf16),
            pltpu.VMEM(conv_b.shape, bf16),
            pltpu.VMEM(conv_c.shape, bf16),
        ),
        in_specs=[hbm] * 29,
        out_specs=(vmem,) * 6,
        scratch_shapes=[
            pltpu.VMEM(tokens.shape, bf16),
            pltpu.VMEM((1, width), f32),
            pltpu.VMEM(w_dt.shape[::-1], bf16),
            pltpu.VMEM((1, heads), f32),
            pltpu.VMEM((1, heads), f32),
            pltpu.VMEM((1, heads), f32),
            pltpu.VMEM(conv_x.shape, bf16),
            pltpu.VMEM(conv_b.shape, bf16),
            pltpu.VMEM(conv_c.shape, bf16),
            pltpu.VMEM(taps_x.shape, bf16),
            pltpu.VMEM(taps_b.shape, bf16),
            pltpu.VMEM(taps_c.shape, bf16),
            pltpu.VMEM((1, w_x.shape[1]), f32),
            pltpu.VMEM((1, width), f32),
            pltpu.VMEM(route_ids.shape, jnp.int32),
            pltpu.VMEM(route_weights.shape, f32),
            pltpu.VMEM((width,), bf16),
            pltpu.VMEM((3, depth, local_hidden), bf16),
            pltpu.VMEM(w_x.shape, bf16),
            pltpu.VMEM(w_z.shape, bf16),
            pltpu.VMEM(w_b.shape, bf16),
            pltpu.VMEM(w_c.shape, bf16),
            pltpu.VMEM(w_out.shape, bf16),
            pltpu.VMEM((width, 2 * hidden), bf16),
            pltpu.VMEM((hidden, width), bf16),
            pltpu.VMEM((heads, seqs, state_dim), f32),
            pltpu.VMEM((splits, seqs, width), bf16),
            pltpu.VMEM((cores, chips, seqs, width + tail), bf16),
            pltpu.VMEM(slab, bf16),
            pltpu.VMEM(slab, bf16),
            pltpu.VMEM((width, 128), bf16),
            pltpu.VMEM((chips * seqs, width), bf16),
            pltpu.VMEM((chips * seqs, width), bf16),
            pltpu.VMEM((splits, chips, seqs, part), bf16),
            dma(17),
            dma(8),
            dma(seqs // 2),
            dma(6),
            dma(splits),
            dma(chips),
            dma(4),
        ],
        compiler_params=pltpu.CompilerParams(
            collective_id=0, has_side_effects=True, vmem_limit_bytes=40 * 2**20
        ),
        cost_estimate=pl.CostEstimate(flops=10**9, bytes_accessed=2 * 10**7, transcendentals=0),
    )(*map(in_hbm, (
        tokens,
        norm1_gain[None],
        conv_x,
        conv_b,
        conv_c,
        w_dt.T,
        dt_bias[None],
        a_log[None],
        d_skip[None],
        taps_x,
        taps_b,
        taps_c,
        group_gain[None],
        norm2_gain[None],
        route_ids,
        route_weights,
        dense_gate,
        dense_up,
        dense_down.T,
        branch_gate,
        ssm_state,
        w_x,
        w_z,
        w_b,
        w_c,
        w_out,
        exp_gate,
        exp_up,
        exp_down,
    )))
    held = [pltpu.with_memory_space_constraint(a, pltpu.VMEM) for a in held]
    shape = jax.ShapeDtypeStruct
    mixed, state, next_x, next_b, next_c = pl.pallas_call(
        finish_kernel,
        out_shape=(
            shape((seqs, part), bf16),
            shape(ssm_state.shape, f32),
            shape(conv_x.shape, bf16),
            shape(conv_b.shape, bf16),
            shape(conv_c.shape, bf16),
        ),
        in_specs=[vmem] * 6,
        out_specs=(hbm,) * 5,
        scratch_shapes=[pltpu.VMEM((seqs, part), bf16), dma(5)],
        compiler_params=pltpu.CompilerParams(vmem_limit_bytes=8 * 2**20),
        cost_estimate=pl.CostEstimate(flops=10**5, bytes_accessed=5 * 10**6, transcendentals=0),
    )(*held)
    return mixed, state, taps_first(next_x), taps_first(next_b), taps_first(next_c)


def solution(mesh):
    return jax.shard_map(
        body,
        mesh=mesh,
        in_specs=(
            P("ep", None),
            P("ep", "tp", None, None),
            P("ep", None, "tp"),
            P("ep", None, "tp"),
            P("ep", None, "tp"),
            P(None, "tp"),
            P(None, "tp"),
            P(None, "tp"),
            P(None, "tp"),
            P(),
            P("tp"),
            P("tp"),
            P("tp"),
            P(None, "tp"),
            P(None, "tp"),
            P(None, "tp"),
            P(),
            P("tp"),
            P("tp", None),
            P(),
            P("ep", None),
            P("ep", None),
            P("ep", None, "tp"),
            P("ep", None, "tp"),
            P("ep", "tp", None),
            P("ep", "tp"),
            P("ep", "tp"),
            P("tp", "ep"),
            P(),
        ),
        out_specs=(
            P("ep", "tp"),
            P("ep", "tp", None, None),
            P("ep", None, "tp"),
            P("ep", None, "tp"),
            P("ep", None, "tp"),
        ),
        check_vma=False,
    )
```

```python
import functools

import jax
import jax.numpy as jnp
from jax import lax
from jax.experimental import pallas as pl
from jax.experimental.pallas import tpu as pltpu
from jax.sharding import PartitionSpec as P

epsilon = 1e-06
cores = 2


def rms_rows(values, gain):
    return values * lax.rsqrt(jnp.mean(values * values, axis=-1, keepdims=True) + epsilon) * gain


def partner(index, i, count):
    if count & (count - 1):
        return lax.rem(index + i, count)
    bit = 1
    other = index
    while bit <= i:
        if i & bit:
            other = other + bit * (1 - 2 * lax.rem(lax.div(index, bit), 2))
        bit *= 2
    return other


def source(index, i, count):
    if count & (count - 1):
        return lax.rem(index + count - i, count)
    return partner(index, i, count)


def layer_kernel(
    peers,
    splits,
    share,
    fold,
    tokens_hbm,
    gain1_hbm,
    prev_x_hbm,
    prev_b_hbm,
    prev_c_hbm,
    wdt_hbm,
    bias_hbm,
    a_log_hbm,
    skip_hbm,
    taps_x_hbm,
    taps_b_hbm,
    taps_c_hbm,
    group_gain_hbm,
    gain2_hbm,
    ids_hbm,
    weights_hbm,
    dense_gate_hbm,
    dense_up_hbm,
    dense_down_hbm,
    branch_hbm,
    state_hbm,
    wx_hbm,
    wz_hbm,
    wb_hbm,
    wc_hbm,
    w_out_hbm,
    gate_hbm,
    up_hbm,
    down_hbm,
    own_ref,
    returned,
    state,
    next_x_ref,
    next_b_ref,
    next_c_ref,
    tokens_ref,
    gain1_ref,
    wdt_ref,
    bias_ref,
    a_log_ref,
    skip_ref,
    prev_x_ref,
    prev_b_ref,
    prev_c_ref,
    taps_x_ref,
    taps_b_ref,
    taps_c_ref,
    group_gain_ref,
    gain2_ref,
    ids_ref,
    weights_ref,
    branch_ref,
    slabs,
    wx,
    wz,
    wb,
    wc,
    w_out,
    gate_up,
    down,
    decays,
    partials,
    features,
    stage_ref,
    arrived,
    dense,
    half_out,
    half_in,
    packed,
    small_sem,
    load_sem,
    in_sem,
    send_sem,
    part_recv,
    feat_recv,
    batch_recv,
):
    ep = lax.axis_index("ep")
    tp = lax.axis_index("tp")
    everyone = peers * splits
    chips = peers // cores
    me = ep * splits + tp
    chip = ep // cores
    core = lax.rem(ep, cores)
    seqs, heads, head_dim, state_dim = state.shape
    width = tokens_ref.shape[1]
    groups = wb.shape[1] // state_dim
    per_group = heads // groups
    inner = heads * head_dim
    hidden = down.shape[0]
    part = width // splits
    depth = slabs.shape[1]

    small = {
        name: pltpu.make_async_copy(hbm, vmem, small_sem.at[i])
        for i, (name, hbm, vmem) in enumerate(
            (
                ("tokens", tokens_hbm, tokens_ref),
                ("gain1", gain1_hbm, gain1_ref),
                ("wdt", wdt_hbm, wdt_ref),
                ("bias", bias_hbm, bias_ref),
                ("a_log", a_log_hbm, a_log_ref),
                ("skip", skip_hbm, skip_ref),
                ("prev_x", prev_x_hbm, prev_x_ref),
                ("taps_x", taps_x_hbm, taps_x_ref),
                ("prev_b", prev_b_hbm, prev_b_ref),
                ("taps_b", taps_b_hbm, taps_b_ref),
                ("prev_c", prev_c_hbm, prev_c_ref),
                ("taps_c", taps_c_hbm, taps_c_ref),
                ("group_gain", group_gain_hbm, group_gain_ref),
                ("gain2", gain2_hbm, gain2_ref),
                ("ids", ids_hbm, ids_ref),
                ("weights", weights_hbm, weights_ref),
                ("branch", branch_hbm, branch_ref),
            )
        )
    }

    def ready(*names):
        for name in names:
            small[name].wait()

    def in_pieces(hbm, vmem, sem, pieces):
        step = vmem.shape[0] // pieces
        return [
            pltpu.make_async_copy(
                hbm.at[pl.ds(i * step, step)], vmem.at[pl.ds(i * step, step)], sem
            )
            for i in range(pieces)
        ]

    wholes = (
        (wx_hbm, wx, 8),
        (wb_hbm, wb, 4),
        (wc_hbm, wc, 4),
        (wz_hbm, wz, 8),
        (w_out_hbm, w_out, 8),
    )
    chunks_of = [in_pieces(a, b, load_sem.at[i], n) for i, (a, b, n) in enumerate(wholes)]
    loaded = [pltpu.make_async_copy(b, b, load_sem.at[i]) for i, (_, b, _) in enumerate(wholes)]
    expert_loads = [
        pltpu.make_async_copy(hbm, vmem, load_sem.at[i])
        for i, hbm, vmem in (
            (5, gate_hbm.at[0], gate_up.at[:, pl.ds(0, hidden)]),
            (5, up_hbm.at[0], gate_up.at[:, pl.ds(hidden, hidden)]),
            (6, down_hbm.at[0], down),
        )
    ]
    slab_loads = [
        pltpu.make_async_copy(hbm, slabs.at[i], load_sem.at[7])
        for i, hbm in enumerate((dense_gate_hbm, dense_up_hbm, dense_down_hbm))
    ]

    fetch_state = [
        pltpu.make_async_copy(
            state_hbm.at[pl.ds(s, 2)], state.at[pl.ds(s, 2)], in_sem.at[s // 2]
        )
        for s in range(0, seqs, 2)
    ]
    for name in ("tokens", "gain1", "wdt", "bias", "a_log", "skip"):
        small[name].start()
    for copy in slab_loads + chunks_of[0]:
        copy.start()
    for name in ("prev_x", "taps_x", "prev_b", "taps_b", "prev_c", "taps_c"):
        small[name].start()

    barrier = pltpu.get_barrier_semaphore()

    def greet(to_ep, to_tp):
        pl.semaphore_signal(
            barrier,
            inc=1,
            device_id={"ep": to_ep, "tp": to_tp},
            device_id_type=pl.DeviceIdType.MESH,
        )

    for i in reversed(range(peers)):
        for j in range(splits):
            if i or j:
                greet(partner(ep, i, peers) if i else ep, partner(tp, j, splits) if j else tp)

    for copy in chunks_of[1] + chunks_of[2]:
        copy.start()
    for name in ("group_gain", "gain2", "ids", "weights", "branch"):
        small[name].start()

    def remote(src, dst, send, recv, to_ep, to_tp):
        return pltpu.make_async_remote_copy(
            src_ref=src,
            dst_ref=dst,
            send_sem=send,
            recv_sem=recv,
            device_id={"ep": to_ep, "tp": to_tp},
            device_id_type=pl.DeviceIdType.MESH,
        )

    mate_ep = cores * chip + 1 - core

    def part_copy(i, slot):
        return remote(
            partials.at[slot],
            partials.at[slot],
            send_sem.at[0],
            part_recv.at[slot],
            ep,
            partner(tp, i, splits),
        )

    def dense_copy(i):
        other = partner(ep, i, peers)
        return remote(
            stage_ref.at[other], arrived.at[ep], send_sem.at[1], batch_recv.at[0], other, tp
        )

    def feat_copy(i, of, slot):
        block = features.at[of, slot]
        return remote(
            block,
            block,
            send_sem.at[2],
            feat_recv.at[of, slot],
            cores * partner(chip, i, chips) + 1,
            tp,
        )

    def pair_copy(of, slot):
        block = features.at[of, slot]
        return remote(block, block, send_sem.at[3], batch_recv.at[1 + of], mate_ep, tp)

    half_copy = remote(half_out, half_in, send_sem.at[4], batch_recv.at[3], mate_ep, tp)

    def ret_copy(i, j):
        to_chip = partner(chip, i, chips) if i else chip
        to_tp = partner(tp, j, splits) if j else tp
        return remote(
            packed.at[to_tp, to_chip],
            returned.at[chip * splits + tp],
            send_sem.at[5],
            batch_recv.at[4],
            cores * to_chip + core,
            to_tp,
        )

    def batch(ref, send, recv):
        return remote(ref, ref, send_sem.at[send], batch_recv.at[recv], mate_ep, tp)

    parts_out = remote(
        partials.at[pl.ds(0, splits - 1)],
        partials.at[pl.ds(0, splits - 1)],
        send_sem.at[0],
        part_recv.at[0],
        mate_ep,
        tp,
    )
    dense_all = batch(arrived.at[pl.ds(0, peers - 1)], 1, 0)
    others = pl.ds(0, chips - 1)
    rets_all = batch(returned.at[pl.ds(0, chips * splits - 1)], 5, 4)

    def project(weights):
        out = jnp.dot(normed, weights, preferred_element_type=jnp.float32)
        return out.astype(jnp.bfloat16).astype(jnp.float32)

    def conv(prev_ref, fresh, taps_ref, next_ref):
        prev = prev_ref[...].astype(jnp.float32)
        taps = taps_ref[...].astype(jnp.float32)
        count = prev.shape[0]
        summed = prev[0] * taps[0:1]
        for j in range(1, count):
            summed = summed + prev[j] * taps[j : j + 1]
            next_ref[j - 1] = prev[j].astype(jnp.bfloat16)
        summed = summed + fresh * taps[count : count + 1]
        next_ref[count - 1] = fresh.astype(jnp.bfloat16)
        return jax.nn.silu(summed)

    high = lambda a: a.astype(jnp.bfloat16).astype(jnp.float32)
    quarter = 4 * ep // peers

    def send_dense():
        for i in reversed(range(1, peers)):
            dense_copy(i).start()

    def meet_and_send(at):
        @pl.when(quarter == at)
        def _():
            pl.semaphore_wait(barrier, everyone - 1)
            send_dense()

    ready("tokens", "gain1", "wdt", "bias", "a_log", "skip")
    for copy in fetch_state:
        copy.start()
    pltpu.make_async_copy(slabs, slabs, load_sem.at[7]).wait()
    normed = rms_rows(tokens_ref[...].astype(jnp.float32), gain1_ref[...]).astype(jnp.bfloat16)
    all_dt = lax.dot_general(
        normed, wdt_ref[...], (((1,), (1,)), ((), ())), preferred_element_type=jnp.float32
    )
    dt_raw = all_dt[:, :heads]
    for t in range(1, all_dt.shape[1] // heads):
        dt_raw = jnp.where(tp == t, all_dt[:, t * heads : (t + 1) * heads], dt_raw)
    step = jax.nn.softplus(dt_raw + bias_ref[...])
    decay = jnp.exp(-step * jnp.exp(a_log_ref[...]))
    for h in range(heads):
        decays[h] = jnp.broadcast_to(decay[:, h : h + 1], (seqs, state_dim))
    spread = lax.broadcasted_iota(jnp.int32, (heads, inner), 1) // head_dim
    spread = spread == lax.broadcasted_iota(jnp.int32, (heads, inner), 0)
    per_head = jnp.concatenate(
        (step, jnp.broadcast_to(skip_ref[...], step.shape), decay), axis=0
    )
    top = high(per_head)
    middle = high(per_head - top)
    pieces = jnp.concatenate((top, middle, per_head - top - middle), axis=0).astype(jnp.bfloat16)
    wide = jnp.dot(pieces, spread.astype(jnp.bfloat16), preferred_element_type=jnp.float32)
    wide = wide[: 3 * seqs] + wide[3 * seqs : 6 * seqs] + wide[6 * seqs :]

    rows = depth // fold
    lane = lax.broadcasted_iota(jnp.int32, (rows, stage_ref.shape[2]), 1)
    for owner in range(peers):
        start = owner * share
        base = start // 128 * 128
        block = []
        for a in range(3):
            found = jnp.zeros(lane.shape, jnp.float32)
            for q in range(fold):
                at = (q if fold > 1 else a) * share
                piece = slabs[a, q * rows : (q + 1) * rows, base : base + 128].astype(jnp.float32)
                shift = (at - (start - base)) % 128
                if shift:
                    piece = pltpu.roll(piece, shift, 1)
                found = jnp.where((lane >= at) & (lane < at + share), piece, found)
            block.append(found)
        if fold > 1:
            for a in range(3):
                stage_ref[owner, a * rows : (a + 1) * rows] = block[a].astype(jnp.bfloat16)
        else:
            stage_ref[owner] = (block[0] + block[1] + block[2]).astype(jnp.bfloat16)
    arrived[ep] = stage_ref[ep]

    loaded[0].wait()
    ready("prev_x", "taps_x")
    xs = conv(prev_x_ref, project(wx[...]), taps_x_ref, next_x_ref)
    for copy in chunks_of[3]:
        copy.start()
    meet_and_send(3)
    loaded[1].wait()
    ready("prev_b", "taps_b")
    bs = conv(prev_b_ref, project(wb[...]), taps_b_ref, next_b_ref)
    loaded[2].wait()
    ready("prev_c", "taps_c")
    cs = conv(prev_c_ref, project(wc[...]), taps_c_ref, next_c_ref)
    stepped = wide[:seqs] * xs
    stepped_high = high(stepped)
    left = jnp.transpose(
        jnp.concatenate((stepped_high, stepped - stepped_high, stepped_high), axis=0)
    ).astype(jnp.bfloat16)
    bs_high = high(bs)
    right = jnp.concatenate((bs_high, bs_high, bs - bs_high), axis=0)
    cs_high = high(cs)
    cs_pair = jnp.concatenate((cs_high, cs - cs_high), axis=0).astype(jnp.bfloat16)
    right_row = lax.rem(lax.broadcasted_iota(jnp.int32, (3 * seqs, state_dim), 0), seqs)
    block = per_group * head_dim
    row = lax.broadcasted_iota(jnp.int32, (seqs, block), 0)
    read = [jnp.zeros((seqs, block), jnp.float32) for _ in range(groups)]
    for s0 in range(0, seqs, 2):
        pair = (s0, s0 + 1)
        if s0 == 2:
            for copy in chunks_of[4]:
                copy.start()
        if s0 == seqs // 2:
            for copy in expert_loads:
                copy.start()
        if s0 == 0:
            meet_and_send(2)
        if s0 == seqs // 2:
            meet_and_send(1)
        fetch_state[s0 // 2].wait()
        for g in range(groups):
            span = slice(g * state_dim, (g + 1) * state_dim)
            old = [state[s, g * per_group : (g + 1) * per_group] for s in pair]
            for k, s in enumerate(pair):
                both = lax.dot_general(
                    cs_pair[:, span],
                    old[k].reshape(block, state_dim).astype(jnp.bfloat16),
                    (((1,), (1,)), ((), ())),
                    preferred_element_type=jnp.float32,
                )
                read[g] = jnp.where(row == s, both[:seqs] + both[seqs:], read[g])
            adders = [jnp.where(right_row == s, right[:, span], 0.0) for s in pair]
            added = jnp.dot(
                left[g * block : (g + 1) * block],
                jnp.concatenate(adders, axis=1).astype(jnp.bfloat16),
                preferred_element_type=jnp.float32,
            )
            for k, s in enumerate(pair):
                for j in range(per_group):
                    h = g * per_group + j
                    state[s, h] = (
                        decays[h, s : s + 1] * old[k][j]
                        + added[
                            j * head_dim : (j + 1) * head_dim, k * state_dim : (k + 1) * state_dim
                        ]
                    )
    met = []
    for g in range(groups):
        span = slice(g * state_dim, (g + 1) * state_dim)
        dots = jnp.sum(bs[:, span] * cs[:, span], axis=1, keepdims=True)
        met.append(jnp.broadcast_to(dots, (seqs, block)))
    readout = wide[2 * seqs :] * jnp.concatenate(read, axis=1)
    readout = readout + stepped * jnp.concatenate(met, axis=1)
    loaded[3].wait()
    gate = jax.nn.silu(project(wz[...]))
    gated = (readout + wide[seqs : 2 * seqs] * xs) * gate
    ready("group_gain", "gain2", "ids", "weights", "branch")
    block = inner // groups
    mixed_heads = []
    for g in range(groups):
        span = slice(g * block, (g + 1) * block)
        piece = gated[:, span]
        piece = piece * lax.rsqrt(jnp.mean(piece * piece, axis=-1, keepdims=True) + epsilon)
        mixed_heads.append((piece * group_gain_ref[:, span]).astype(jnp.bfloat16))
    loaded[4].wait()
    partial_out = jnp.dot(
        jnp.concatenate(mixed_heads, axis=1), w_out[...], preferred_element_type=jnp.float32
    )
    partials[tp] = partial_out.astype(jnp.bfloat16)

    @pl.when(quarter == 0)
    def _():
        pl.semaphore_wait(barrier, everyone - 1)

    for i in range(1, splits):
        part_copy(i, tp).start()
    pl.when(quarter == 0)(send_dense)

    tail = features.shape[3] - width
    lanes = lax.broadcasted_iota(jnp.int32, (seqs, tail), 1)
    table = jnp.zeros((seqs, tail), jnp.float32)
    for k in range(ids_ref.shape[1]):
        table = table + jnp.where(
            lax.rem(lanes, peers) == ids_ref[:, k : k + 1], weights_ref[:, k : k + 1], 0.0
        )
    table = jnp.where(lanes < peers, high(table), table - high(table))
    features[core, chip, :, width:] = table.astype(jnp.bfloat16)

    for i in range(1, splits):
        part_copy(i, source(tp, i, splits)).wait_recv()
    summed = partials[0].astype(jnp.float32)
    for t in range(1, splits):
        summed = summed + partials[t].astype(jnp.float32)
    residual = (tokens_ref[...].astype(jnp.float32) + summed).astype(jnp.bfloat16)
    residual = residual.astype(jnp.float32)
    features[core, chip, :, :width] = rms_rows(residual, gain2_ref[...]).astype(jnp.bfloat16)
    for i in reversed(range(1, chips)):
        feat_copy(i, core, chip).start()

    @pl.when(core == 0)
    def _():
        remote(
            features.at[0, chip],
            features.at[0, chip],
            send_sem.at[2],
            feat_recv.at[0, chip],
            mate_ep,
            tp,
        ).start()

    @pl.when(core == 1)
    def _():
        pair_copy(1, chip).start()

    own_rows = residual[:, :part]
    for t in range(1, splits):
        own_rows = jnp.where(tp == t, residual[:, t * part : (t + 1) * part], own_rows)
    own_ref[...] = own_rows

    def collect(of, first, last):
        for i in range(first, last):
            slot = source(chip, i, chips)
            feat_copy(i, of, slot).wait_recv()
            pair_copy(of, slot).start()

    @pl.when(core == 1)
    def _():
        collect(1, 1, chips // 2)

    dense_all.wait_recv()
    if fold > 1:
        for s in range(peers):
            for q in range(fold):
                found = jnp.zeros(lane.shape, jnp.float32)
                for a in range(3):
                    piece = arrived[s, a * rows : (a + 1) * rows].astype(jnp.float32)
                    shift = (a - q) * share % 128
                    if shift:
                        piece = pltpu.roll(piece, shift, 1)
                    found = jnp.where(
                        (lane >= a * share) & (lane < (a + 1) * share), piece, found
                    )
                at = s * depth + q * rows
                dense[at : at + rows] = found.astype(jnp.bfloat16)
        dense_weights = dense[...]
    else:
        dense_weights = arrived[...].reshape(width, arrived.shape[2])
    @pl.when(core == 1)
    def _():
        collect(1, chips // 2, chips)
        feat_copy(1, 0, chip).wait_recv()
        collect(0, 1, chips)

    @pl.when(core == 0)
    def _():
        batch(features.at[1], 3, 2).wait_recv()

    pltpu.make_async_copy(gate_up, gate_up, load_sem.at[5]).wait()
    expert_loads[2].wait()
    rows_of = chips * seqs
    branch_row = branch_ref[...].astype(jnp.float32).reshape(1, width)

    def feed_forward(of):
        rows16 = features[of, :, :, :width].reshape(rows_of, width)
        weights = features[of, :, :, width:].reshape(rows_of, tail).astype(jnp.float32)
        columns = lax.broadcasted_iota(jnp.int32, weights.shape, 1)
        columns = (columns == ep) | (columns == ep + peers)
        weight = jnp.sum(jnp.where(columns, weights, 0.0), axis=1, keepdims=True)
        pre = jnp.dot(rows16, gate_up[...], preferred_element_type=jnp.float32)
        active = weight * (jax.nn.silu(pre[:, :hidden]) * pre[:, hidden:])
        dense_pre = jnp.dot(rows16, dense_weights, preferred_element_type=jnp.float32)
        branch = jax.nn.sigmoid(
            jnp.sum(rows16.astype(jnp.float32) * branch_row, axis=1, keepdims=True)
        )
        lane = lax.broadcasted_iota(jnp.int32, dense_pre.shape, 1)
        dense_act = jax.nn.silu(pltpu.roll(dense_pre, 2 * share, 1))
        dense_act = dense_act * pltpu.roll(dense_pre, share, 1)
        dense_act = jnp.where((lane >= 2 * share) & (lane < 3 * share), branch * dense_act, 0.0)
        total = jnp.dot(active.astype(jnp.bfloat16), down[...], preferred_element_type=jnp.float32)
        return total + lax.dot_general(
            dense_act.astype(jnp.bfloat16),
            dense_weights,
            (((1,), (1,)), ((), ())),
            preferred_element_type=jnp.float32,
        )

    half_out[...] = feed_forward(1 - core).astype(jnp.bfloat16)
    half_copy.start()

    @pl.when(core == 0)
    def _():
        batch(features.at[0, others], 3, 1).wait_recv()

    total = feed_forward(core)
    half_copy.wait_recv()
    total = total + half_in[...].astype(jnp.float32)
    for t in range(splits):
        packed[t] = (
            total[:, t * part : (t + 1) * part].reshape(chips, seqs, part).astype(jnp.bfloat16)
        )
    for i in reversed(range(chips)):
        for j in reversed(range(splits)):
            if i or j:
                ret_copy(i, j).start()
    returned[chip * splits + tp] = packed[tp, chip]

    parts_out.wait_send()
    dense_all.wait_send()

    @pl.when(core == 0)
    def _():
        batch(features.at[0], 2, 1).wait_send()

    @pl.when(core == 1)
    def _():
        batch(features.at[0, others], 2, 1).wait_send()
        batch(features.at[0, others], 3, 1).wait_send()
        batch(features.at[1], 3, 1).wait_send()

    half_copy.wait_send()
    rets_all.wait_recv()
    rets_all.wait_send()


def finish_kernel(
    own_ref, returned, state, x_ref, b_ref, c_ref, out_ref, state_out, x_out, b_out, c_out, sum_ref, sem
):
    seqs = state.shape[0]
    for s in range(seqs):
        pltpu.make_async_copy(state.at[s], state_out.at[s], sem.at[0]).start()
    puts = [pltpu.make_async_copy(state, state_out, sem.at[0])]
    for i, (ref, out) in enumerate(((x_ref, x_out), (b_ref, b_out), (c_ref, c_out))):
        puts.append(pltpu.make_async_copy(ref, out, sem.at[1 + i]))
        puts[-1].start()
    mixed = own_ref[...] + jnp.sum(returned[...].astype(jnp.float32), axis=0)
    sum_ref[...] = mixed.astype(jnp.bfloat16)
    puts.append(pltpu.make_async_copy(sum_ref, out_ref, sem.at[4]))
    puts[-1].start()
    for put in puts:
        put.wait()


def body(
    tokens,
    ssm_state,
    conv_x,
    conv_b,
    conv_c,
    w_x,
    w_z,
    w_b,
    w_c,
    w_dt,
    dt_bias,
    a_log,
    d_skip,
    taps_x,
    taps_b,
    taps_c,
    norm1_gain,
    group_gain,
    w_out,
    norm2_gain,
    route_ids,
    route_weights,
    exp_gate,
    exp_up,
    exp_down,
    dense_gate,
    dense_up,
    dense_down,
    branch_gate,
):
    peers = lax.axis_size("ep")
    splits = lax.axis_size("tp")
    chips = peers // cores
    seqs, width = tokens.shape
    depth, local_hidden = dense_gate.shape
    share = local_hidden // peers
    hidden = exp_gate.shape[2]
    part = width // splits
    heads, state_dim = ssm_state.shape[1], ssm_state.shape[3]
    fold = 128 // share
    if share * fold != 128 or depth % (16 * fold):
        fold = 1
    slab = (peers, 3 * depth // fold if fold > 1 else depth, 128)
    tail = -(-2 * peers // 128) * 128
    vmem = pl.BlockSpec(memory_space=pltpu.VMEM)
    hbm = pl.BlockSpec(memory_space=pltpu.HBM)
    dma = lambda count: pltpu.SemaphoreType.DMA((count,))
    taps_first = lambda a: a.transpose(1, 0, 2)
    conv_x, conv_b, conv_c = taps_first(conv_x), taps_first(conv_b), taps_first(conv_c)
    bf16, f32 = jnp.bfloat16, jnp.float32
    in_hbm = lambda a: pltpu.with_memory_space_constraint(a, pltpu.HBM)
    held = pl.pallas_call(
        functools.partial(layer_kernel, peers, splits, share, fold),
        out_shape=(
            pltpu.VMEM((seqs, part), f32),
            pltpu.VMEM((chips * splits, seqs, part), bf16),
            pltpu.VMEM(ssm_state.shape, f32),
            pltpu.VMEM(conv_x.shape, bf16),
            pltpu.VMEM(conv_b.shape, bf16),
            pltpu.VMEM(conv_c.shape, bf16),
        ),
        in_specs=[hbm] * 29,
        out_specs=(vmem,) * 6,
        scratch_shapes=[
            pltpu.VMEM(tokens.shape, bf16),
            pltpu.VMEM((1, width), f32),
            pltpu.VMEM(w_dt.shape[::-1], bf16),
            pltpu.VMEM((1, heads), f32),
            pltpu.VMEM((1, heads), f32),
            pltpu.VMEM((1, heads), f32),
            pltpu.VMEM(conv_x.shape, bf16),
            pltpu.VMEM(conv_b.shape, bf16),
            pltpu.VMEM(conv_c.shape, bf16),
            pltpu.VMEM(taps_x.shape, bf16),
            pltpu.VMEM(taps_b.shape, bf16),
            pltpu.VMEM(taps_c.shape, bf16),
            pltpu.VMEM((1, w_x.shape[1]), f32),
            pltpu.VMEM((1, width), f32),
            pltpu.VMEM(route_ids.shape, jnp.int32),
            pltpu.VMEM(route_weights.shape, f32),
            pltpu.VMEM((width,), bf16),
            pltpu.VMEM((3, depth, local_hidden), bf16),
            pltpu.VMEM(w_x.shape, bf16),
            pltpu.VMEM(w_z.shape, bf16),
            pltpu.VMEM(w_b.shape, bf16),
            pltpu.VMEM(w_c.shape, bf16),
            pltpu.VMEM(w_out.shape, bf16),
            pltpu.VMEM((width, 2 * hidden), bf16),
            pltpu.VMEM((hidden, width), bf16),
            pltpu.VMEM((heads, seqs, state_dim), f32),
            pltpu.VMEM((splits, seqs, width), bf16),
            pltpu.VMEM((cores, chips, seqs, width + tail), bf16),
            pltpu.VMEM(slab, bf16),
            pltpu.VMEM(slab, bf16),
            pltpu.VMEM((width, 128), bf16),
            pltpu.VMEM((chips * seqs, width), bf16),
            pltpu.VMEM((chips * seqs, width), bf16),
            pltpu.VMEM((splits, chips, seqs, part), bf16),
            dma(17),
            dma(8),
            dma(seqs // 2),
            dma(6),
            dma(splits),
            pltpu.SemaphoreType.DMA((cores, chips)),
            dma(5),
        ],
        compiler_params=pltpu.CompilerParams(
            collective_id=0, has_side_effects=True, vmem_limit_bytes=40 * 2**20
        ),
        cost_estimate=pl.CostEstimate(flops=10**9, bytes_accessed=2 * 10**7, transcendentals=0),
    )(*map(in_hbm, (
        tokens,
        norm1_gain[None],
        conv_x,
        conv_b,
        conv_c,
        w_dt.T,
        dt_bias[None],
        a_log[None],
        d_skip[None],
        taps_x,
        taps_b,
        taps_c,
        group_gain[None],
        norm2_gain[None],
        route_ids,
        route_weights,
        dense_gate,
        dense_up,
        dense_down.T,
        branch_gate,
        ssm_state,
        w_x,
        w_z,
        w_b,
        w_c,
        w_out,
        exp_gate,
        exp_up,
        exp_down,
    )))
    held = [pltpu.with_memory_space_constraint(a, pltpu.VMEM) for a in held]
    shape = jax.ShapeDtypeStruct
    mixed, state, next_x, next_b, next_c = pl.pallas_call(
        finish_kernel,
        out_shape=(
            shape((seqs, part), bf16),
            shape(ssm_state.shape, f32),
            shape(conv_x.shape, bf16),
            shape(conv_b.shape, bf16),
            shape(conv_c.shape, bf16),
        ),
        in_specs=[vmem] * 6,
        out_specs=(hbm,) * 5,
        scratch_shapes=[pltpu.VMEM((seqs, part), bf16), dma(5)],
        compiler_params=pltpu.CompilerParams(vmem_limit_bytes=8 * 2**20),
        cost_estimate=pl.CostEstimate(flops=10**5, bytes_accessed=5 * 10**6, transcendentals=0),
    )(*held)
    return mixed, state, taps_first(next_x), taps_first(next_b), taps_first(next_c)


def solution(mesh):
    return jax.shard_map(
        body,
        mesh=mesh,
        in_specs=(
            P("ep", None),
            P("ep", "tp", None, None),
            P("ep", None, "tp"),
            P("ep", None, "tp"),
            P("ep", None, "tp"),
            P(None, "tp"),
            P(None, "tp"),
            P(None, "tp"),
            P(None, "tp"),
            P(),
            P("tp"),
            P("tp"),
            P("tp"),
            P(None, "tp"),
            P(None, "tp"),
            P(None, "tp"),
            P(),
            P("tp"),
            P("tp", None),
            P(),
            P("ep", None),
            P("ep", None),
            P("ep", None, "tp"),
            P("ep", None, "tp"),
            P("ep", "tp", None),
            P("ep", "tp"),
            P("ep", "tp"),
            P("tp", "ep"),
            P(),
        ),
        out_specs=(
            P("ep", "tp"),
            P("ep", "tp", None, None),
            P("ep", None, "tp"),
            P("ep", None, "tp"),
            P("ep", None, "tp"),
        ),
        check_vma=False,
    )
```

```python
import functools

import jax
import jax.numpy as jnp
from jax import lax
from jax.experimental import pallas as pl
from jax.experimental.pallas import tpu as pltpu
from jax.sharding import PartitionSpec as P

epsilon = 1e-06
cores = 2


def rms_rows(values, gain):
    return values * lax.rsqrt(jnp.mean(values * values, axis=-1, keepdims=True) + epsilon) * gain


def partner(index, i, count):
    if count & (count - 1):
        return lax.rem(index + i, count)
    bit = 1
    other = index
    while bit <= i:
        if i & bit:
            other = other + bit * (1 - 2 * lax.rem(lax.div(index, bit), 2))
        bit *= 2
    return other


def source(index, i, count):
    if count & (count - 1):
        return lax.rem(index + count - i, count)
    return partner(index, i, count)


def layer_kernel(
    peers,
    splits,
    share,
    fold,
    tokens_hbm,
    gain1_hbm,
    prev_x_hbm,
    prev_b_hbm,
    prev_c_hbm,
    wdt_hbm,
    bias_hbm,
    a_log_hbm,
    skip_hbm,
    taps_x_hbm,
    taps_b_hbm,
    taps_c_hbm,
    group_gain_hbm,
    gain2_hbm,
    ids_hbm,
    weights_hbm,
    dense_gate_hbm,
    dense_up_hbm,
    dense_down_hbm,
    branch_hbm,
    state_hbm,
    wx_hbm,
    wz_hbm,
    wb_hbm,
    wc_hbm,
    w_out_hbm,
    gate_hbm,
    up_hbm,
    down_hbm,
    own_ref,
    returned,
    state,
    next_x_ref,
    next_b_ref,
    next_c_ref,
    tokens_ref,
    gain1_ref,
    wdt_ref,
    bias_ref,
    a_log_ref,
    skip_ref,
    prev_x_ref,
    prev_b_ref,
    prev_c_ref,
    taps_x_ref,
    taps_b_ref,
    taps_c_ref,
    group_gain_ref,
    gain2_ref,
    ids_ref,
    weights_ref,
    branch_ref,
    slabs,
    wx,
    wz,
    wb,
    wc,
    w_out,
    gate_up,
    down,
    decays,
    partials,
    features,
    stage_ref,
    arrived,
    dense,
    half_out,
    half_in,
    packed,
    small_sem,
    load_sem,
    in_sem,
    send_sem,
    part_recv,
    feat_recv,
    batch_recv,
):
    ep = lax.axis_index("ep")
    tp = lax.axis_index("tp")
    everyone = peers * splits
    chips = peers // cores
    me = ep * splits + tp
    chip = ep // cores
    core = lax.rem(ep, cores)
    seqs, heads, head_dim, state_dim = state.shape
    width = tokens_ref.shape[1]
    groups = wb.shape[1] // state_dim
    per_group = heads // groups
    inner = heads * head_dim
    hidden = down.shape[0]
    part = width // splits
    depth = slabs.shape[1]

    small = {
        name: pltpu.make_async_copy(hbm, vmem, small_sem.at[i])
        for i, (name, hbm, vmem) in enumerate(
            (
                ("tokens", tokens_hbm, tokens_ref),
                ("gain1", gain1_hbm, gain1_ref),
                ("wdt", wdt_hbm, wdt_ref),
                ("bias", bias_hbm, bias_ref),
                ("a_log", a_log_hbm, a_log_ref),
                ("skip", skip_hbm, skip_ref),
                ("prev_x", prev_x_hbm, prev_x_ref),
                ("taps_x", taps_x_hbm, taps_x_ref),
                ("prev_b", prev_b_hbm, prev_b_ref),
                ("taps_b", taps_b_hbm, taps_b_ref),
                ("prev_c", prev_c_hbm, prev_c_ref),
                ("taps_c", taps_c_hbm, taps_c_ref),
                ("group_gain", group_gain_hbm, group_gain_ref),
                ("gain2", gain2_hbm, gain2_ref),
                ("ids", ids_hbm, ids_ref),
                ("weights", weights_hbm, weights_ref),
                ("branch", branch_hbm, branch_ref),
            )
        )
    }

    def ready(*names):
        for name in names:
            small[name].wait()

    def in_pieces(hbm, vmem, sem, pieces):
        step = vmem.shape[0] // pieces
        return [
            pltpu.make_async_copy(
                hbm.at[pl.ds(i * step, step)], vmem.at[pl.ds(i * step, step)], sem
            )
            for i in range(pieces)
        ]

    wholes = (
        (wx_hbm, wx, 8),
        (wb_hbm, wb, 4),
        (wc_hbm, wc, 4),
        (wz_hbm, wz, 8),
        (w_out_hbm, w_out, 8),
    )
    chunks_of = [in_pieces(a, b, load_sem.at[i], n) for i, (a, b, n) in enumerate(wholes)]
    loaded = [pltpu.make_async_copy(b, b, load_sem.at[i]) for i, (_, b, _) in enumerate(wholes)]
    expert_loads = [
        pltpu.make_async_copy(hbm, vmem, load_sem.at[i])
        for i, hbm, vmem in (
            (5, gate_hbm.at[0], gate_up.at[:, pl.ds(0, hidden)]),
            (5, up_hbm.at[0], gate_up.at[:, pl.ds(hidden, hidden)]),
            (6, down_hbm.at[0], down),
        )
    ]
    slab_loads = [
        pltpu.make_async_copy(hbm, slabs.at[i], load_sem.at[7])
        for i, hbm in enumerate((dense_gate_hbm, dense_up_hbm, dense_down_hbm))
    ]

    fetch_state = [
        pltpu.make_async_copy(
            state_hbm.at[pl.ds(s, 2)], state.at[pl.ds(s, 2)], in_sem.at[s // 2]
        )
        for s in range(0, seqs, 2)
    ]
    for name in ("tokens", "gain1", "wdt", "bias", "a_log", "skip"):
        small[name].start()
    for copy in slab_loads + chunks_of[0]:
        copy.start()
    for name in ("prev_x", "taps_x", "prev_b", "taps_b", "prev_c", "taps_c"):
        small[name].start()

    barrier = pltpu.get_barrier_semaphore()

    def greet(to_ep, to_tp):
        pl.semaphore_signal(
            barrier,
            inc=1,
            device_id={"ep": to_ep, "tp": to_tp},
            device_id_type=pl.DeviceIdType.MESH,
        )

    for i in reversed(range(peers)):
        for j in range(splits):
            if i or j:
                greet(partner(ep, i, peers) if i else ep, partner(tp, j, splits) if j else tp)

    for copy in chunks_of[1] + chunks_of[2]:
        copy.start()
    for name in ("group_gain", "gain2", "ids", "weights", "branch"):
        small[name].start()

    def remote(src, dst, send, recv, to_ep, to_tp):
        return pltpu.make_async_remote_copy(
            src_ref=src,
            dst_ref=dst,
            send_sem=send,
            recv_sem=recv,
            device_id={"ep": to_ep, "tp": to_tp},
            device_id_type=pl.DeviceIdType.MESH,
        )

    mate_ep = cores * chip + 1 - core

    def part_copy(i, slot):
        return remote(
            partials.at[slot],
            partials.at[slot],
            send_sem.at[0],
            part_recv.at[slot],
            ep,
            partner(tp, i, splits),
        )

    def dense_copy(i):
        other = partner(ep, i, peers)
        return remote(
            stage_ref.at[other], arrived.at[ep], send_sem.at[1], batch_recv.at[0], other, tp
        )

    def feat_copy(i, of, slot):
        block = features.at[of, slot]
        return remote(
            block,
            block,
            send_sem.at[2],
            feat_recv.at[of, slot],
            cores * partner(chip, i, chips) + 1,
            tp,
        )

    def pair_copy(of, slot):
        block = features.at[of, slot]
        return remote(block, block, send_sem.at[3], batch_recv.at[1 + of], mate_ep, tp)

    half_copy = remote(half_out, half_in, send_sem.at[4], batch_recv.at[3], mate_ep, tp)

    def ret_copy(i, j):
        to_chip = partner(chip, i, chips) if i else chip
        to_tp = partner(tp, j, splits) if j else tp
        return remote(
            packed.at[to_tp, to_chip],
            returned.at[chip * splits + tp],
            send_sem.at[5],
            batch_recv.at[4],
            cores * to_chip + core,
            to_tp,
        )

    def batch(ref, send, recv):
        return remote(ref, ref, send_sem.at[send], batch_recv.at[recv], mate_ep, tp)

    parts_out = remote(
        partials.at[pl.ds(0, splits - 1)],
        partials.at[pl.ds(0, splits - 1)],
        send_sem.at[0],
        part_recv.at[0],
        mate_ep,
        tp,
    )
    dense_all = batch(arrived.at[pl.ds(0, peers - 1)], 1, 0)
    others = pl.ds(0, chips - 1)
    rets_all = batch(returned.at[pl.ds(0, chips * splits - 1)], 5, 4)

    def project(weights):
        out = jnp.dot(normed, weights, preferred_element_type=jnp.float32)
        return out.astype(jnp.bfloat16).astype(jnp.float32)

    def conv(prev_ref, fresh, taps_ref, next_ref):
        prev = prev_ref[...].astype(jnp.float32)
        taps = taps_ref[...].astype(jnp.float32)
        count = prev.shape[0]
        summed = prev[0] * taps[0:1]
        for j in range(1, count):
            summed = summed + prev[j] * taps[j : j + 1]
            next_ref[j - 1] = prev[j].astype(jnp.bfloat16)
        summed = summed + fresh * taps[count : count + 1]
        next_ref[count - 1] = fresh.astype(jnp.bfloat16)
        return jax.nn.silu(summed)

    high = lambda a: a.astype(jnp.bfloat16).astype(jnp.float32)
    quarter = 4 * ep // peers

    def send_dense():
        for i in reversed(range(1, peers)):
            dense_copy(i).start()

    def meet_and_send(at):
        @pl.when(quarter == at)
        def _():
            pl.semaphore_wait(barrier, everyone - 1)
            send_dense()

    ready("tokens", "gain1", "wdt", "bias", "a_log", "skip")
    for copy in fetch_state:
        copy.start()
    pltpu.make_async_copy(slabs, slabs, load_sem.at[7]).wait()
    normed = rms_rows(tokens_ref[...].astype(jnp.float32), gain1_ref[...]).astype(jnp.bfloat16)
    all_dt = lax.dot_general(
        normed, wdt_ref[...], (((1,), (1,)), ((), ())), preferred_element_type=jnp.float32
    )
    dt_raw = all_dt[:, :heads]
    for t in range(1, all_dt.shape[1] // heads):
        dt_raw = jnp.where(tp == t, all_dt[:, t * heads : (t + 1) * heads], dt_raw)
    step = jax.nn.softplus(dt_raw + bias_ref[...])
    decay = jnp.exp(-step * jnp.exp(a_log_ref[...]))
    for h in range(heads):
        decays[h] = jnp.broadcast_to(decay[:, h : h + 1], (seqs, state_dim))
    spread = lax.broadcasted_iota(jnp.int32, (heads, inner), 1) // head_dim
    spread = spread == lax.broadcasted_iota(jnp.int32, (heads, inner), 0)
    per_head = jnp.concatenate(
        (step, jnp.broadcast_to(skip_ref[...], step.shape), decay), axis=0
    )
    top = high(per_head)
    middle = high(per_head - top)
    pieces = jnp.concatenate((top, middle, per_head - top - middle), axis=0).astype(jnp.bfloat16)
    wide = jnp.dot(pieces, spread.astype(jnp.bfloat16), preferred_element_type=jnp.float32)
    wide = wide[: 3 * seqs] + wide[3 * seqs : 6 * seqs] + wide[6 * seqs :]

    rows = depth // fold
    lane = lax.broadcasted_iota(jnp.int32, (rows, stage_ref.shape[2]), 1)
    for owner in range(peers):
        start = owner * share
        base = start // 128 * 128
        block = []
        for a in range(3):
            found = jnp.zeros(lane.shape, jnp.float32)
            for q in range(fold):
                at = (q if fold > 1 else a) * share
                piece = slabs[a, q * rows : (q + 1) * rows, base : base + 128].astype(jnp.float32)
                shift = (at - (start - base)) % 128
                if shift:
                    piece = pltpu.roll(piece, shift, 1)
                found = jnp.where((lane >= at) & (lane < at + share), piece, found)
            block.append(found)
        if fold > 1:
            for a in range(3):
                stage_ref[owner, a * rows : (a + 1) * rows] = block[a].astype(jnp.bfloat16)
        else:
            stage_ref[owner] = (block[0] + block[1] + block[2]).astype(jnp.bfloat16)
    arrived[ep] = stage_ref[ep]

    loaded[0].wait()
    ready("prev_x", "taps_x")
    xs = conv(prev_x_ref, project(wx[...]), taps_x_ref, next_x_ref)
    for copy in chunks_of[3]:
        copy.start()
    meet_and_send(3)
    loaded[1].wait()
    ready("prev_b", "taps_b")
    bs = conv(prev_b_ref, project(wb[...]), taps_b_ref, next_b_ref)
    loaded[2].wait()
    ready("prev_c", "taps_c")
    cs = conv(prev_c_ref, project(wc[...]), taps_c_ref, next_c_ref)
    stepped = wide[:seqs] * xs
    stepped_high = high(stepped)
    left = jnp.transpose(
        jnp.concatenate((stepped_high, stepped - stepped_high, stepped_high), axis=0)
    ).astype(jnp.bfloat16)
    bs_high = high(bs)
    right = jnp.concatenate((bs_high, bs_high, bs - bs_high), axis=0)
    cs_high = high(cs)
    cs_pair = jnp.concatenate((cs_high, cs - cs_high), axis=0).astype(jnp.bfloat16)
    right_row = lax.rem(lax.broadcasted_iota(jnp.int32, (3 * seqs, state_dim), 0), seqs)
    block = per_group * head_dim
    row = lax.broadcasted_iota(jnp.int32, (seqs, block), 0)
    read = [jnp.zeros((seqs, block), jnp.float32) for _ in range(groups)]
    for s0 in range(0, seqs, 2):
        pair = (s0, s0 + 1)
        if s0 == 2:
            for copy in chunks_of[4]:
                copy.start()
        if s0 == seqs // 2:
            for copy in expert_loads:
                copy.start()
        if s0 == 0:
            meet_and_send(2)
            meet_and_send(1)
        fetch_state[s0 // 2].wait()
        for g in range(groups):
            span = slice(g * state_dim, (g + 1) * state_dim)
            old = [state[s, g * per_group : (g + 1) * per_group] for s in pair]
            for k, s in enumerate(pair):
                both = lax.dot_general(
                    cs_pair[:, span],
                    old[k].reshape(block, state_dim).astype(jnp.bfloat16),
                    (((1,), (1,)), ((), ())),
                    preferred_element_type=jnp.float32,
                )
                read[g] = jnp.where(row == s, both[:seqs] + both[seqs:], read[g])
            adders = [jnp.where(right_row == s, right[:, span], 0.0) for s in pair]
            added = jnp.dot(
                left[g * block : (g + 1) * block],
                jnp.concatenate(adders, axis=1).astype(jnp.bfloat16),
                preferred_element_type=jnp.float32,
            )
            for k, s in enumerate(pair):
                for j in range(per_group):
                    h = g * per_group + j
                    state[s, h] = (
                        decays[h, s : s + 1] * old[k][j]
                        + added[
                            j * head_dim : (j + 1) * head_dim, k * state_dim : (k + 1) * state_dim
                        ]
                    )
    met = []
    for g in range(groups):
        span = slice(g * state_dim, (g + 1) * state_dim)
        dots = jnp.sum(bs[:, span] * cs[:, span], axis=1, keepdims=True)
        met.append(jnp.broadcast_to(dots, (seqs, block)))
    readout = wide[2 * seqs :] * jnp.concatenate(read, axis=1)
    readout = readout + stepped * jnp.concatenate(met, axis=1)
    loaded[3].wait()
    gate = jax.nn.silu(project(wz[...]))
    gated = (readout + wide[seqs : 2 * seqs] * xs) * gate
    ready("group_gain", "gain2", "ids", "weights", "branch")
    block = inner // groups
    mixed_heads = []
    for g in range(groups):
        span = slice(g * block, (g + 1) * block)
        piece = gated[:, span]
        piece = piece * lax.rsqrt(jnp.mean(piece * piece, axis=-1, keepdims=True) + epsilon)
        mixed_heads.append((piece * group_gain_ref[:, span]).astype(jnp.bfloat16))
    loaded[4].wait()
    partial_out = jnp.dot(
        jnp.concatenate(mixed_heads, axis=1), w_out[...], preferred_element_type=jnp.float32
    )
    partials[tp] = partial_out.astype(jnp.bfloat16)

    @pl.when(quarter == 0)
    def _():
        pl.semaphore_wait(barrier, everyone - 1)

    for i in range(1, splits):
        part_copy(i, tp).start()
    pl.when(quarter == 0)(send_dense)

    tail = features.shape[3] - width
    lanes = lax.broadcasted_iota(jnp.int32, (seqs, tail), 1)
    table = jnp.zeros((seqs, tail), jnp.float32)
    for k in range(ids_ref.shape[1]):
        table = table + jnp.where(
            lax.rem(lanes, peers) == ids_ref[:, k : k + 1], weights_ref[:, k : k + 1], 0.0
        )
    table = jnp.where(lanes < peers, high(table), table - high(table))
    features[core, chip, :, width:] = table.astype(jnp.bfloat16)

    for i in range(1, splits):
        part_copy(i, source(tp, i, splits)).wait_recv()
    summed = partials[0].astype(jnp.float32)
    for t in range(1, splits):
        summed = summed + partials[t].astype(jnp.float32)
    residual = (tokens_ref[...].astype(jnp.float32) + summed).astype(jnp.bfloat16)
    residual = residual.astype(jnp.float32)
    features[core, chip, :, :width] = rms_rows(residual, gain2_ref[...]).astype(jnp.bfloat16)
    for i in reversed(range(1, chips)):
        feat_copy(i, core, chip).start()

    @pl.when(core == 0)
    def _():
        remote(
            features.at[0, chip],
            features.at[0, chip],
            send_sem.at[2],
            feat_recv.at[0, chip],
            mate_ep,
            tp,
        ).start()

    @pl.when(core == 1)
    def _():
        pair_copy(1, chip).start()

    own_rows = residual[:, :part]
    for t in range(1, splits):
        own_rows = jnp.where(tp == t, residual[:, t * part : (t + 1) * part], own_rows)
    own_ref[...] = own_rows

    def collect(of, first, last):
        for i in range(first, last):
            slot = source(chip, i, chips)
            feat_copy(i, of, slot).wait_recv()
            pair_copy(of, slot).start()

    @pl.when(core == 1)
    def _():
        collect(1, 1, chips // 2)

    dense_all.wait_recv()
    if fold > 1:
        for s in range(peers):
            for q in range(fold):
                found = jnp.zeros(lane.shape, jnp.float32)
                for a in range(3):
                    piece = arrived[s, a * rows : (a + 1) * rows].astype(jnp.float32)
                    shift = (a - q) * share % 128
                    if shift:
                        piece = pltpu.roll(piece, shift, 1)
                    found = jnp.where(
                        (lane >= a * share) & (lane < (a + 1) * share), piece, found
                    )
                at = s * depth + q * rows
                dense[at : at + rows] = found.astype(jnp.bfloat16)
        dense_weights = dense[...]
    else:
        dense_weights = arrived[...].reshape(width, arrived.shape[2])
    @pl.when(core == 1)
    def _():
        collect(1, chips // 2, chips)
        feat_copy(1, 0, chip).wait_recv()
        collect(0, 1, chips)

    @pl.when(core == 0)
    def _():
        batch(features.at[1], 3, 2).wait_recv()

    pltpu.make_async_copy(gate_up, gate_up, load_sem.at[5]).wait()
    expert_loads[2].wait()
    rows_of = chips * seqs
    branch_row = branch_ref[...].astype(jnp.float32).reshape(1, width)

    def feed_forward(of):
        rows16 = features[of, :, :, :width].reshape(rows_of, width)
        weights = features[of, :, :, width:].reshape(rows_of, tail).astype(jnp.float32)
        columns = lax.broadcasted_iota(jnp.int32, weights.shape, 1)
        columns = (columns == ep) | (columns == ep + peers)
        weight = jnp.sum(jnp.where(columns, weights, 0.0), axis=1, keepdims=True)
        pre = jnp.dot(rows16, gate_up[...], preferred_element_type=jnp.float32)
        active = weight * (jax.nn.silu(pre[:, :hidden]) * pre[:, hidden:])
        dense_pre = jnp.dot(rows16, dense_weights, preferred_element_type=jnp.float32)
        branch = jax.nn.sigmoid(
            jnp.sum(rows16.astype(jnp.float32) * branch_row, axis=1, keepdims=True)
        )
        lane = lax.broadcasted_iota(jnp.int32, dense_pre.shape, 1)
        dense_act = jax.nn.silu(pltpu.roll(dense_pre, 2 * share, 1))
        dense_act = dense_act * pltpu.roll(dense_pre, share, 1)
        dense_act = jnp.where((lane >= 2 * share) & (lane < 3 * share), branch * dense_act, 0.0)
        total = jnp.dot(active.astype(jnp.bfloat16), down[...], preferred_element_type=jnp.float32)
        return total + lax.dot_general(
            dense_act.astype(jnp.bfloat16),
            dense_weights,
            (((1,), (1,)), ((), ())),
            preferred_element_type=jnp.float32,
        )

    half_out[...] = feed_forward(1 - core).astype(jnp.bfloat16)
    half_copy.start()

    @pl.when(core == 0)
    def _():
        batch(features.at[0, others], 3, 1).wait_recv()

    total = feed_forward(core)
    half_copy.wait_recv()
    total = total + half_in[...].astype(jnp.float32)
    for t in range(splits):
        packed[t] = (
            total[:, t * part : (t + 1) * part].reshape(chips, seqs, part).astype(jnp.bfloat16)
        )
    for i in reversed(range(chips)):
        for j in reversed(range(splits)):
            if i or j:
                ret_copy(i, j).start()
    returned[chip * splits + tp] = packed[tp, chip]

    parts_out.wait_send()
    dense_all.wait_send()

    @pl.when(core == 0)
    def _():
        batch(features.at[0], 2, 1).wait_send()

    @pl.when(core == 1)
    def _():
        batch(features.at[0, others], 2, 1).wait_send()
        batch(features.at[0, others], 3, 1).wait_send()
        batch(features.at[1], 3, 1).wait_send()

    half_copy.wait_send()
    rets_all.wait_recv()
    rets_all.wait_send()


def finish_kernel(
    own_ref, returned, state, x_ref, b_ref, c_ref, out_ref, state_out, x_out, b_out, c_out, sum_ref, sem
):
    seqs = state.shape[0]
    for s in range(seqs):
        pltpu.make_async_copy(state.at[s], state_out.at[s], sem.at[0]).start()
    puts = [pltpu.make_async_copy(state, state_out, sem.at[0])]
    for i, (ref, out) in enumerate(((x_ref, x_out), (b_ref, b_out), (c_ref, c_out))):
        puts.append(pltpu.make_async_copy(ref, out, sem.at[1 + i]))
        puts[-1].start()
    mixed = own_ref[...] + jnp.sum(returned[...].astype(jnp.float32), axis=0)
    sum_ref[...] = mixed.astype(jnp.bfloat16)
    puts.append(pltpu.make_async_copy(sum_ref, out_ref, sem.at[4]))
    puts[-1].start()
    for put in puts:
        put.wait()


def body(
    tokens,
    ssm_state,
    conv_x,
    conv_b,
    conv_c,
    w_x,
    w_z,
    w_b,
    w_c,
    w_dt,
    dt_bias,
    a_log,
    d_skip,
    taps_x,
    taps_b,
    taps_c,
    norm1_gain,
    group_gain,
    w_out,
    norm2_gain,
    route_ids,
    route_weights,
    exp_gate,
    exp_up,
    exp_down,
    dense_gate,
    dense_up,
    dense_down,
    branch_gate,
):
    peers = lax.axis_size("ep")
    splits = lax.axis_size("tp")
    chips = peers // cores
    seqs, width = tokens.shape
    depth, local_hidden = dense_gate.shape
    share = local_hidden // peers
    hidden = exp_gate.shape[2]
    part = width // splits
    heads, state_dim = ssm_state.shape[1], ssm_state.shape[3]
    fold = 128 // share
    if share * fold != 128 or depth % (16 * fold):
        fold = 1
    slab = (peers, 3 * depth // fold if fold > 1 else depth, 128)
    tail = -(-2 * peers // 128) * 128
    vmem = pl.BlockSpec(memory_space=pltpu.VMEM)
    hbm = pl.BlockSpec(memory_space=pltpu.HBM)
    dma = lambda count: pltpu.SemaphoreType.DMA((count,))
    taps_first = lambda a: a.transpose(1, 0, 2)
    conv_x, conv_b, conv_c = taps_first(conv_x), taps_first(conv_b), taps_first(conv_c)
    bf16, f32 = jnp.bfloat16, jnp.float32
    in_hbm = lambda a: pltpu.with_memory_space_constraint(a, pltpu.HBM)
    held = pl.pallas_call(
        functools.partial(layer_kernel, peers, splits, share, fold),
        out_shape=(
            pltpu.VMEM((seqs, part), f32),
            pltpu.VMEM((chips * splits, seqs, part), bf16),
            pltpu.VMEM(ssm_state.shape, f32),
            pltpu.VMEM(conv_x.shape, bf16),
            pltpu.VMEM(conv_b.shape, bf16),
            pltpu.VMEM(conv_c.shape, bf16),
        ),
        in_specs=[hbm] * 29,
        out_specs=(vmem,) * 6,
        scratch_shapes=[
            pltpu.VMEM(tokens.shape, bf16),
            pltpu.VMEM((1, width), f32),
            pltpu.VMEM(w_dt.shape[::-1], bf16),
            pltpu.VMEM((1, heads), f32),
            pltpu.VMEM((1, heads), f32),
            pltpu.VMEM((1, heads), f32),
            pltpu.VMEM(conv_x.shape, bf16),
            pltpu.VMEM(conv_b.shape, bf16),
            pltpu.VMEM(conv_c.shape, bf16),
            pltpu.VMEM(taps_x.shape, bf16),
            pltpu.VMEM(taps_b.shape, bf16),
            pltpu.VMEM(taps_c.shape, bf16),
            pltpu.VMEM((1, w_x.shape[1]), f32),
            pltpu.VMEM((1, width), f32),
            pltpu.VMEM(route_ids.shape, jnp.int32),
            pltpu.VMEM(route_weights.shape, f32),
            pltpu.VMEM((width,), bf16),
            pltpu.VMEM((3, depth, local_hidden), bf16),
            pltpu.VMEM(w_x.shape, bf16),
            pltpu.VMEM(w_z.shape, bf16),
            pltpu.VMEM(w_b.shape, bf16),
            pltpu.VMEM(w_c.shape, bf16),
            pltpu.VMEM(w_out.shape, bf16),
            pltpu.VMEM((width, 2 * hidden), bf16),
            pltpu.VMEM((hidden, width), bf16),
            pltpu.VMEM((heads, seqs, state_dim), f32),
            pltpu.VMEM((splits, seqs, width), bf16),
            pltpu.VMEM((cores, chips, seqs, width + tail), bf16),
            pltpu.VMEM(slab, bf16),
            pltpu.VMEM(slab, bf16),
            pltpu.VMEM((width, 128), bf16),
            pltpu.VMEM((chips * seqs, width), bf16),
            pltpu.VMEM((chips * seqs, width), bf16),
            pltpu.VMEM((splits, chips, seqs, part), bf16),
            dma(17),
            dma(8),
            dma(seqs // 2),
            dma(6),
            dma(splits),
            pltpu.SemaphoreType.DMA((cores, chips)),
            dma(5),
        ],
        compiler_params=pltpu.CompilerParams(
            collective_id=0, has_side_effects=True, vmem_limit_bytes=40 * 2**20
        ),
        cost_estimate=pl.CostEstimate(flops=10**9, bytes_accessed=2 * 10**7, transcendentals=0),
    )(*map(in_hbm, (
        tokens,
        norm1_gain[None],
        conv_x,
        conv_b,
        conv_c,
        w_dt.T,
        dt_bias[None],
        a_log[None],
        d_skip[None],
        taps_x,
        taps_b,
        taps_c,
        group_gain[None],
        norm2_gain[None],
        route_ids,
        route_weights,
        dense_gate,
        dense_up,
        dense_down.T,
        branch_gate,
        ssm_state,
        w_x,
        w_z,
        w_b,
        w_c,
        w_out,
        exp_gate,
        exp_up,
        exp_down,
    )))
    held = [pltpu.with_memory_space_constraint(a, pltpu.VMEM) for a in held]
    shape = jax.ShapeDtypeStruct
    mixed, state, next_x, next_b, next_c = pl.pallas_call(
        finish_kernel,
        out_shape=(
            shape((seqs, part), bf16),
            shape(ssm_state.shape, f32),
            shape(conv_x.shape, bf16),
            shape(conv_b.shape, bf16),
            shape(conv_c.shape, bf16),
        ),
        in_specs=[vmem] * 6,
        out_specs=(hbm,) * 5,
        scratch_shapes=[pltpu.VMEM((seqs, part), bf16), dma(5)],
        compiler_params=pltpu.CompilerParams(vmem_limit_bytes=8 * 2**20),
        cost_estimate=pl.CostEstimate(flops=10**5, bytes_accessed=5 * 10**6, transcendentals=0),
    )(*held)
    return mixed, state, taps_first(next_x), taps_first(next_b), taps_first(next_c)


def solution(mesh):
    return jax.shard_map(
        body,
        mesh=mesh,
        in_specs=(
            P("ep", None),
            P("ep", "tp", None, None),
            P("ep", None, "tp"),
            P("ep", None, "tp"),
            P("ep", None, "tp"),
            P(None, "tp"),
            P(None, "tp"),
            P(None, "tp"),
            P(None, "tp"),
            P(),
            P("tp"),
            P("tp"),
            P("tp"),
            P(None, "tp"),
            P(None, "tp"),
            P(None, "tp"),
            P(),
            P("tp"),
            P("tp", None),
            P(),
            P("ep", None),
            P("ep", None),
            P("ep", None, "tp"),
            P("ep", None, "tp"),
            P("ep", "tp", None),
            P("ep", "tp"),
            P("ep", "tp"),
            P("tp", "ep"),
            P(),
        ),
        out_specs=(
            P("ep", "tp"),
            P("ep", "tp", None, None),
            P("ep", None, "tp"),
            P("ep", None, "tp"),
            P("ep", None, "tp"),
        ),
        check_vma=False,
    )
```
